32 devices in a mesh: ep: 4 (over y, x), tp: 8 (over z, core).
Axes of the slice: x: 2, y: 2, z: 4, core: 2. Of those that a mesh axis runs over, the one named last changes fastest.
Arguments:
- queries: bfloat16 [2048, 16, 128], P('ep', 'tp'), may hold values from -300 to 300
- keys: bfloat16 [2048, 16, 128], P('ep', 'tp'), may hold values from -4 to 4
- values: bfloat16 [2048, 16, 128], P('ep', 'tp'), may hold values from -6 to 6
- mix_weight: float32 [16], P('tp'), may hold values from 0.3 to 0.8
- sub_gain: float32 [128], replicated, may hold values from 0.1 to 1.9
- tokens: bfloat16 [1024, 2048], P('ep', 'tp'), may hold values from -6 to 6
- routes: int32 [1024, 2], P('ep'), may hold values from 0 to 7, all different within a row; in each aligned block of 256 rows (0 to 255, 256 to 511, ...) at most 96 rows name the same one
- route_weights: float32 [1024, 2], P('ep'), may hold values from 0.1 to 1
- expert_gain: float32 [2048], replicated, may hold values from 0.1 to 1.9
- gate_weight: bfloat16 [8, 2048, 4096], P('ep', None, 'tp'), may hold values from -0.375 to 0.375
- up_weight: bfloat16 [8, 2048, 4096], P('ep', None, 'tp'), may hold values from -0.375 to 0.375
- down_weight: bfloat16 [8, 4096, 2048], P('ep', 'tp'), may hold values from -0.09375 to 0.09375
Outputs:
- attn_out: bfloat16 [2048, 16, 128], P('ep', 'tp')
- moe_out: bfloat16 [1024, 2048], P('ep', 'tp')
The draws below stay inside these ranges and needn't reach their ends.
Inputs may be any that keep to these rules, and one draw needn't show every extreme that they name: `routes`: in each aligned block of 256 rows no expert is named by more than 96 rows, and in every draw some expert is named by exactly 96 rows of some block.
All inputs are finite; a program needn't handle non-finite values.
Results may differ from the reference program's by a relative error of at most 0.018.
Values may be sent and summed in bfloat16 or wider, within the bound.
No kernel may reach another device: no remote copies, remote signals or barrier semaphores. Data moves between devices by JAX's collectives and lax.ppermute only.
A program may use at most 128 MiB of HBM per device.

```python
import math
import jax
import jax.numpy as jnp
import numpy as np
from jax import lax

D = 2048
HEADS = 16
HEAD_QK = 64
HEAD_V = 128
FF = 4096
TOPK = 2
ROWS2 = 256
LENGTH = 2048
TOKENS2 = 1024
EXPERTS = 8
CAP = 96
N_EP = 4
N_TP = 8


def paired_fields(key):
    base = jax.random.fold_in(key, 31)
    query_key, field_key = jax.random.split(base, 2)
    shape = (LENGTH, HEADS, 2, HEAD_QK)
    queries = 1.8 * jax.random.truncated_normal(query_key, -4.0, 4.0, shape, jnp.float32)
    keys = jax.random.truncated_normal(field_key, -4.0, 4.0, shape, jnp.float32)
    return (queries.reshape(LENGTH, HEADS, 2 * HEAD_QK), keys.reshape(LENGTH, HEADS, 2 * HEAD_QK))


def draw_queries(key, part):
    return paired_fields(key)[0].astype(jnp.bfloat16)


def draw_keys(key, part):
    return paired_fields(key)[1].astype(jnp.bfloat16)


def block_scale(rng, dims, cuts, smallest, largest):
    def one(axis_at, shards_of):
        draws = jax.random.uniform(jax.random.fold_in(jax.random.fold_in(rng, 6), axis_at), (shards_of,), jnp.float32, smallest / len(cuts), largest / len(cuts))
        return jnp.repeat(jnp.exp(draws), dims[axis_at] // shards_of).reshape((-1,) + (1,) * (len(dims) - axis_at - 1))

    factor_of = one(*cuts[0])
    for cut in cuts[1:]:
        factor_of = factor_of * one(*cut)
    return factor_of


def assign_block(stream_key, own, number, rows, number_of, top, limit, lean):
    order = jax.random.permutation(stream_key, number_of)
    heavy_load, usual = shares(number_of, rows * top, limit, lean, True), shares(number_of, rows * top, limit, lean, False)
    places = jnp.arange(number_of)

    def named(sizes, offset_by):
        used = int((sizes > 0).sum())
        fixed = max(1, used // 4)
        moved = fixed + (places - fixed + offset_by * (used - fixed)) % max(1, number_of - fixed)
        return jnp.zeros((number_of,), jnp.int32).at[order[jnp.where(places < fixed, places, moved)]].set(jnp.asarray(sizes, jnp.int32))

    sizes = jnp.where(number % 4 == 0, named(heavy_load, number // 4), named(usual, number - number // 4 - 1))
    mixed = jax.random.permutation(jax.random.fold_in(own, 3), number_of)
    source_of, sink = mixed[0:number_of // 2 * 2:2], mixed[1:number_of // 2 * 2:2]
    margin = jnp.minimum(sizes[source_of] - 1, limit - sizes[sink]) // 2
    margin = jnp.where((source_of == order[0]) | (sink == order[0]) | (sizes[sink] == 0), 0, jnp.maximum(margin, 0))
    moved = jax.random.randint(jax.random.fold_in(own, 4), (number_of // 2,), 0, 1 << 20) % (margin + 1)
    sizes = sizes.at[source_of].add(-moved).at[sink].add(moved)
    labels = jnp.searchsorted(jnp.cumsum(sizes), jnp.arange(rows * top), side="right").astype(jnp.int32)
    listing = labels.reshape(top, rows).T
    listing = listing[jax.random.permutation(jax.random.fold_in(own, 1), rows)]
    offset_by = jax.random.randint(jax.random.fold_in(own, 2), (rows, 1), 0, top)
    return jnp.take_along_axis(listing, (jnp.arange(top)[None, :] + offset_by) % top, axis=1)


def shares(number_of, total, most, slope, full):
    loads = [(1 << 20) // math.isqrt(grade ** slope) + 1 for grade in range(1, number_of + 1)]
    largest = most if full else min(most, max(-(-total // number_of), total * loads[0] // sum(loads)))
    least = 1 if total - largest >= number_of - 1 else 0
    counts, surplus = [largest] + [least] * (number_of - 1), total - largest - least * (number_of - 1)
    while surplus > 0:
        movable = [i for i in range(1, number_of) if counts[i] < largest] or [i for i in range(1, number_of) if counts[i] < most]
        pool, remaining = sum([loads[i] for i in movable]), surplus
        for i in movable:
            extra = min(most - counts[i], max(1, remaining * loads[i] // pool), surplus)
            counts[i] = counts[i] + extra
            surplus = surplus - extra
    return np.array(counts)


def bell_draw(key, extent, width, bound, pieces=(), kind=jnp.bfloat16):
    entries = jax.random.normal(key, extent, jnp.float32) * width
    if len(pieces) > 0:
        entries = block_scale(key, extent, pieces, -0.22, 0.18) * entries
    return jnp.clip(entries, min=-bound, max=bound).astype(kind)


def setup_inputs(seed: int = 0) -> dict:
    arg_keys = jax.random.split(jax.random.key(seed), 13)
    queries = draw_queries(jax.random.fold_in(arg_keys[12], 71), 0)
    keys = draw_keys(jax.random.fold_in(arg_keys[12], 71), 0)
    values = bell_draw(arg_keys[2], (LENGTH, HEADS, HEAD_V), 1.0, 6.0, ((0, 4), (1, 8)))
    mix_weight = jnp.clip(0.3 + 0.5 * jax.random.uniform(arg_keys[3], (HEADS,), jnp.float32) ** block_scale(arg_keys[3], (HEADS,), ((0, 8),), -0.2, 0.2), 0.3, 0.8)
    sub_gain = jnp.clip(1.0 + 0.18 * jax.random.normal(arg_keys[4], (HEAD_V,), jnp.float32), 0.1, 1.9)
    tokens = bell_draw(arg_keys[5], (TOKENS2, D), 1.0, 6.0, ((0, 4), (1, 8)))
    routes_keys = jax.random.split(jax.random.fold_in(arg_keys[6], 1), TOKENS2 // ROWS2)
    routes_turns = jax.random.permutation(jax.random.fold_in(arg_keys[6], 3), TOKENS2 // ROWS2)
    routes = jax.vmap(lambda own, number: assign_block(jax.random.fold_in(arg_keys[6], 2), own, number, ROWS2, EXPERTS, TOPK, CAP, 1))(routes_keys, routes_turns).reshape((TOKENS2, TOPK))
    route_weights = jnp.clip(0.1 + 0.9 * jax.random.uniform(arg_keys[7], (TOKENS2, TOPK), jnp.float32) ** block_scale(arg_keys[7], (TOKENS2, TOPK), ((0, 4),), -0.2, 0.2), 0.1, 1.0)
    expert_gain = jnp.clip(1.0 + 0.18 * jax.random.normal(arg_keys[8], (D,), jnp.float32), 0.1, 1.9)
    gate_weight = bell_draw(arg_keys[9], (EXPERTS, D, FF), (D // 9) ** -0.5, 0.375, ((0, 4), (2, 8)))
    up_weight = bell_draw(arg_keys[10], (EXPERTS, D, FF), (D // 9) ** -0.5, 0.375, ((0, 4), (2, 8)))
    down_weight = bell_draw(arg_keys[11], (EXPERTS, FF, D), FF ** -0.5, 0.09375, ((0, 4), (1, 8)))
    return {"queries": queries, "keys": keys, "values": values, "mix_weight": mix_weight, "sub_gain": sub_gain, "tokens": tokens, "routes": routes, "route_weights": route_weights, "expert_gain": expert_gain, "gate_weight": gate_weight, "up_weight": up_weight, "down_weight": down_weight}


NEG_FILL = -1e+30
SUB_EPS = 1e-05
NORM_EPS = 1e-06
CLAMP_LIMIT = 7.0
GLU_ALPHA = 1.702
OUT_SCALE = 0.8

def head_attention(bundle, sub_gain):
    head_queries, head_keys, head_values, mix_value = bundle
    block_size = math.gcd(LENGTH, 512)
    key_all = head_keys.reshape(LENGTH, 2, HEAD_QK).astype(jnp.float32)
    key_pos = jnp.arange(LENGTH, dtype=jnp.int32)

    def one_block(block_index):
        offset = block_index * block_size
        query_block = lax.dynamic_slice_in_dim(head_queries, offset, block_size, 0)
        query_block = query_block.reshape(block_size, 2, HEAD_QK).astype(jnp.float32)
        scores = jnp.einsum('qmd,kmd->mqk', query_block, key_all) * HEAD_QK ** (-0.5)
        query_pos = offset + jnp.arange(block_size, dtype=jnp.int32)
        visible = key_pos[None, :] <= query_pos[:, None]
        row_max = lax.optimization_barrier(jnp.max(jnp.where(visible, scores, NEG_FILL), axis=-1))
        weights = jnp.where(visible, jnp.exp(scores - row_max[..., None]), 0.0)
        row_sum = lax.optimization_barrier(jnp.sum(weights, axis=-1))
        rounded = weights.astype(jnp.bfloat16)
        first = jnp.dot(rounded[0], head_values, preferred_element_type=jnp.float32) / row_sum[0][:, None]
        second = jnp.dot(rounded[1], head_values, preferred_element_type=jnp.float32) / row_sum[1][:, None]
        blend = first - mix_value * second
        scaled = blend * lax.rsqrt(lax.optimization_barrier(jnp.mean(blend * blend, axis=-1, keepdims=True)) + SUB_EPS)
        return (scaled * sub_gain * OUT_SCALE).astype(jnp.bfloat16)
    outputs = lax.map(one_block, jnp.arange(LENGTH // block_size, dtype=jnp.int32))
    return outputs.reshape(LENGTH, HEAD_V)

def reference(queries, keys, values, mix_weight, sub_gain, tokens, routes, route_weights, expert_gain, gate_weight, up_weight, down_weight):

    def per_head(bundle):
        return head_attention(bundle, sub_gain)
    heads_all = lax.map(per_head, (jnp.transpose(queries, (1, 0, 2)), jnp.transpose(keys, (1, 0, 2)), jnp.transpose(values, (1, 0, 2)), mix_weight))
    attn_out = jnp.transpose(heads_all, (1, 0, 2))
    floats = tokens.astype(jnp.float32)
    factor = lax.rsqrt(lax.optimization_barrier(jnp.mean(floats * floats, axis=-1)) + NORM_EPS)
    normed = (floats * expert_gain).astype(jnp.bfloat16)
    block_routes = routes.reshape(N_EP, ROWS2 * TOPK)
    onehot = (block_routes[..., None] == jnp.arange(EXPERTS, dtype=jnp.int32)[None, None, :]).astype(jnp.int32)
    slot_rank = lax.optimization_barrier(jnp.sum((jnp.cumsum(onehot, axis=1) - 1) * onehot, axis=2)).astype(jnp.int32)
    target = block_routes * CAP + slot_rank
    token_ids = (jnp.arange(N_EP, dtype=jnp.int32)[:, None] * ROWS2 + jnp.arange(ROWS2 * TOPK, dtype=jnp.int32)[None, :] // TOPK).astype(jnp.int32)
    block_ids = jnp.broadcast_to(jnp.arange(N_EP, dtype=jnp.int32)[:, None], target.shape)
    slot_owner = jnp.full((N_EP, EXPERTS * CAP), TOKENS2, jnp.int32).at[block_ids, target].set(token_ids)
    slot_owner = jnp.transpose(slot_owner.reshape(N_EP, EXPERTS, CAP), (1, 0, 2)).reshape(EXPERTS, N_EP * CAP)
    padded_rows = jnp.concatenate([normed, jnp.zeros((1, D), jnp.bfloat16)], axis=0)
    padded_factor = jnp.concatenate([factor, jnp.zeros((1,), jnp.float32)], axis=0)

    def run_expert(bundle):
        slot_list, expert_gate, expert_up, expert_down = bundle
        rows_in = padded_rows[slot_list]
        scale = padded_factor[slot_list][:, None]
        gate_pre = jnp.minimum(jnp.dot(rows_in, expert_gate, preferred_element_type=jnp.float32) * scale, CLAMP_LIMIT)
        up_pre = jnp.clip(jnp.dot(rows_in, expert_up, preferred_element_type=jnp.float32) * scale, -CLAMP_LIMIT, CLAMP_LIMIT)
        hidden = ((up_pre + 1.0) * gate_pre * jax.nn.sigmoid(GLU_ALPHA * gate_pre)).astype(jnp.bfloat16)
        hidden_parts = hidden.reshape(N_EP * CAP, N_TP, FF // N_TP)
        down_parts = expert_down.reshape(N_TP, FF // N_TP, D)

        def add_part(part_index, running):
            piece = jnp.dot(hidden_parts[:, part_index], down_parts[part_index], preferred_element_type=jnp.float32).astype(jnp.bfloat16)
            piece = lax.optimization_barrier(piece)
            return running + piece.astype(jnp.float32)
        summed = lax.fori_loop(0, N_TP, add_part, jnp.zeros((N_EP * CAP, D), jnp.float32))
        return summed.astype(jnp.bfloat16)
    expert_rows = lax.map(run_expert, (slot_owner, gate_weight, up_weight, down_weight)).reshape(EXPERTS, N_EP, CAP, D)
    row_block = (jnp.arange(TOKENS2, dtype=jnp.int32) // ROWS2)[:, None]
    picked = expert_rows[routes, jnp.broadcast_to(row_block, routes.shape), slot_rank.reshape(TOKENS2, TOPK)]
    moe_out = lax.optimization_barrier(jnp.sum(picked.astype(jnp.float32) * route_weights[..., None], axis=1)).astype(jnp.bfloat16)
    return (attn_out, moe_out)
```

```python
import functools

import jax
import jax.numpy as jnp
from jax import lax
from jax.experimental import pallas as pl
from jax.experimental.pallas import tpu as pltpu
from jax.sharding import PartitionSpec as P

NEG_FILL = -1e30
SUB_EPS = 1e-05
NORM_EPS = 1e-06
CLAMP_LIMIT = 7.0
GLU_ALPHA = 1.702
OUT_SCALE = 0.8
LOG2E = 1.4426950408889634
CORES = 2

VMEM = pltpu.VMEM
SMEM = pltpu.SMEM


def whole():
    return pl.BlockSpec(memory_space=VMEM)


def scalars():
    return pl.BlockSpec(memory_space=SMEM)


def core_groups(size):
    return [[CORES * level + core for level in range(size // CORES)] for core in range(CORES)]


def swap_core(value):
    pairs = [(source, source ^ 1) for source in range(lax.axis_size("tp"))]
    return lax.ppermute(value, "tp", pairs)


def exchange_levels(value):
    groups = core_groups(lax.axis_size("tp"))
    return lax.all_to_all(
        value, "tp", split_axis=0, concat_axis=0, axis_index_groups=groups, tiled=True
    )


def exchange_groups(value):
    return lax.all_to_all(value, "ep", split_axis=0, concat_axis=0, tiled=True)


def attention_kernel(spot_ref, mix_ref, bundle_ref, gain_ref, out_ref, scores, *, rows, scale):
    blocks, _, width = bundle_ref.shape
    share = out_ref.shape[1]
    splits = rows // share
    head, part = spot_ref[0], spot_ref[1]
    mix = mix_ref[head]
    half = width // 2
    lane = lax.broadcasted_iota(jnp.int32, (share, width), 1)
    row = lax.broadcasted_iota(jnp.int32, (share, rows), 0)
    column = lax.broadcasted_iota(jnp.int32, (share, rows), 1)
    contract = (((1,), (1,)), ((), ()))
    factor = scale * LOG2E
    for block in range(blocks):
        place = part if block % 2 == 0 else splits - 1 - part
        visible = column <= row + place * share
        queries = bundle_ref[block, 2 * rows :, :]
        sums = []
        for side in range(2):
            own = (lane < half) if side == 0 else (lane >= half)
            query = jnp.where(own, queries, jnp.zeros_like(queries))
            top = jnp.full((share, 1), NEG_FILL, jnp.float32)
            for other in range(block + 1):
                score = lax.dot_general(
                    query,
                    bundle_ref[other, :rows, :],
                    contract,
                    preferred_element_type=jnp.float32,
                )
                if other == block:
                    score = jnp.where(visible, score, NEG_FILL)
                scores[side, :, other * rows : (other + 1) * rows] = score
                top = jnp.maximum(top, jnp.max(score, axis=-1, keepdims=True))
            total = jnp.zeros((share, 1), jnp.float32)
            weighted = jnp.zeros((share, width), jnp.float32)
            for other in range(block + 1):
                score = scores[side, :, other * rows : (other + 1) * rows]
                weight = jnp.exp2((score - top) * factor)
                total += jnp.sum(weight, axis=-1, keepdims=True)
                weighted += jnp.dot(
                    weight.astype(jnp.bfloat16),
                    bundle_ref[other, rows : 2 * rows, :],
                    preferred_element_type=jnp.float32,
                )
            sums.append(weighted / total)
        blend = sums[0] - mix * sums[1]
        mean = jnp.mean(blend * blend, axis=-1, keepdims=True)
        scaled = blend * lax.rsqrt(mean + SUB_EPS)
        out_ref[block] = (scaled * gain_ref[...] * OUT_SCALE).astype(out_ref.dtype)


def attend_pack(queries, keys, values):
    rows, heads, width = queries.shape
    groups = lax.axis_size("ep")
    splits = groups // heads
    share = rows // splits
    odd = lax.axis_index("ep") % 2 == 1
    by_head = [jnp.transpose(value, (1, 0, 2)) for value in (queries, keys, values)]
    shares = by_head[0].reshape(heads, splits, share, width)
    shares = jnp.where(odd, shares[:, ::-1], shares)
    wide = (heads, splits, rows, width)
    bundle = jnp.concatenate(
        [
            jnp.broadcast_to(by_head[1][:, None], wide),
            jnp.broadcast_to(by_head[2][:, None], wide),
            shares,
        ],
        axis=2,
    )
    return bundle.reshape(groups, 2 * rows + share, width)


def attend_compute(bundle, mix_weight, sub_gain, rows):
    groups, tall, width = bundle.shape
    share = tall - 2 * rows
    splits = rows // share
    place = lax.axis_index("ep")
    spot = jnp.stack([place // splits, place % splits]).astype(jnp.int32)
    pairs = groups * (groups + 1) // 2 * share * rows * 2
    return pl.pallas_call(
        functools.partial(attention_kernel, rows=rows, scale=(width // 2) ** -0.5),
        out_shape=jax.ShapeDtypeStruct((groups, share, width), jnp.bfloat16),
        in_specs=[scalars(), scalars(), whole(), whole()],
        out_specs=whole(),
        scratch_shapes=[pltpu.VMEM((2, share, groups * rows), jnp.float32)],
        cost_estimate=pl.CostEstimate(
            flops=pairs * 4 * width, bytes_accessed=bundle.size * 2, transcendentals=pairs
        ),
        name="attention",
    )(spot, mix_weight, bundle, sub_gain[None, :])


def attend_unpack(returned, heads):
    groups, share, width = returned.shape
    splits = groups // heads
    odd = lax.axis_index("ep") % 2 == 1
    shares = returned.reshape(heads, splits, share, width)
    shares = jnp.where(odd, shares[:, ::-1], shares)
    return jnp.transpose(shares.reshape(heads, splits * share, width), (1, 0, 2))


def dispatch_kernel(routes_ref, rows_ref, *out_refs, capacity, pieces, experts):
    levels, rows, width = rows_ref.shape
    picks = routes_ref.shape[0]
    tall = max(experts, 16)
    expert = lax.broadcasted_iota(jnp.int32, (tall, rows), 0)
    named = jnp.zeros((tall, rows), jnp.bool_)
    for pick in range(picks):
        named = named | (routes_ref[pick : pick + 1, :] == expert)
    earlier = (
        lax.broadcasted_iota(jnp.int32, (rows, rows), 0)
        < lax.broadcasted_iota(jnp.int32, (rows, rows), 1)
    ).astype(jnp.float32)
    rank = jnp.dot(
        named.astype(jnp.float32).astype(jnp.bfloat16),
        earlier.astype(jnp.bfloat16),
        preferred_element_type=jnp.float32,
    )
    slots = (experts // pieces) * capacity
    slot = lax.broadcasted_iota(jnp.int32, (slots, rows), 0)
    for piece in range(pieces):
        chosen = jnp.zeros((slots, rows), jnp.bool_)
        for pick in range(picks):
            route = routes_ref[pick : pick + 1, :]
            mine = jnp.sum(jnp.where(expert == route, rank, 0.0), axis=0, keepdims=True)
            target = lax.div(route, pieces) * capacity + mine.astype(jnp.int32)
            target = jnp.where(lax.rem(route, pieces) == piece, target, -1)
            chosen = chosen | (slot == target)
        onehot = chosen.astype(jnp.float32).astype(jnp.bfloat16)
        for level in range(levels):
            out_refs[piece][:, level * width : (level + 1) * width] = jnp.dot(
                onehot, rows_ref[level], preferred_element_type=jnp.float32
            ).astype(jnp.bfloat16)


def dispatch(routes, by_level, capacity, pieces, experts):
    levels, rows, width = by_level.shape
    slots = experts // pieces * capacity
    return pl.pallas_call(
        functools.partial(dispatch_kernel, capacity=capacity, pieces=pieces, experts=experts),
        out_shape=[jax.ShapeDtypeStruct((slots, levels * width), jnp.bfloat16)] * pieces,
        in_specs=[whole(), whole()],
        out_specs=[whole()] * pieces,
        cost_estimate=pl.CostEstimate(
            flops=2 * slots * pieces * rows * levels * width,
            bytes_accessed=4 * slots * pieces * levels * width,
            transcendentals=0,
        ),
        name="dispatch",
    )(routes.T, by_level)


def expert_kernel(
    core_ref, own_ref, other_ref, gain_ref, gate_ref, up_ref, down_ref,
    kept_ref, sent_ref, normed, factor, hidden, *, width,
):
    step = pl.program_id(0)
    core = core_ref[0]
    levels = own_ref.shape[1] // width
    total_width = levels * CORES * width
    tile = gate_ref.shape[2]

    def column(level, side):
        start = (CORES * level + (core if side == 0 else 1 - core)) * width
        return pl.ds(pl.multiple_of(start, width), width)

    @pl.when(step == 0)
    def _():
        squares = jnp.zeros((own_ref.shape[0], 1), jnp.float32)
        for side, ref in ((0, own_ref), (1, other_ref)):
            for level in range(levels):
                floats = ref[:, level * width : (level + 1) * width].astype(jnp.float32)
                squares += jnp.sum(floats * floats, axis=-1, keepdims=True)
                place = column(level, side)
                normed[:, place] = (floats * gain_ref[:, place]).astype(jnp.bfloat16)
        factor[...] = lax.rsqrt(squares / total_width + NORM_EPS)

    gate = jnp.dot(normed[...], gate_ref[0], preferred_element_type=jnp.float32)
    up = jnp.dot(normed[...], up_ref[0], preferred_element_type=jnp.float32)
    gate = jnp.minimum(gate * factor[...], CLAMP_LIMIT)
    up = jnp.clip(up * factor[...], -CLAMP_LIMIT, CLAMP_LIMIT)
    value = ((up + 1.0) * gate * jax.nn.sigmoid(GLU_ALPHA * gate)).astype(jnp.bfloat16)
    hidden[:, pl.ds(pl.multiple_of(step * tile, tile), tile)] = value

    @pl.when(step == pl.num_programs(0) - 1)
    def _():
        for side, ref in ((1, sent_ref), (0, kept_ref)):
            for level in range(levels):
                ref[:, level * width : (level + 1) * width] = jnp.dot(
                    hidden[...],
                    down_ref[0, :, column(level, side)],
                    preferred_element_type=jnp.float32,
                ).astype(jnp.bfloat16)


def run_expert(piece, own, other, gain, gate_weight, up_weight, down_weight, width):
    slots, half = own.shape
    _, total_width, ff = gate_weight.shape
    tile = ff // 2 if ff % 512 == 0 else ff
    core = (lax.axis_index("tp") % CORES).astype(jnp.int32)[None]
    return pl.pallas_call(
        functools.partial(expert_kernel, width=width),
        out_shape=[jax.ShapeDtypeStruct((slots, half), jnp.bfloat16)] * 2,
        grid=(ff // tile,),
        in_specs=[
            scalars(),
            pl.BlockSpec((slots, half), lambda i: (0, 0)),
            pl.BlockSpec((slots, half), lambda i: (0, 0)),
            pl.BlockSpec((1, total_width), lambda i: (0, 0)),
            pl.BlockSpec((1, total_width, tile), lambda i: (piece, 0, i)),
            pl.BlockSpec((1, total_width, tile), lambda i: (piece, 0, i)),
            pl.BlockSpec((1, ff, total_width), lambda i: (piece, 0, 0)),
        ],
        out_specs=[pl.BlockSpec((slots, half), lambda i: (0, 0))] * 2,
        scratch_shapes=[
            pltpu.VMEM((slots, total_width), jnp.bfloat16),
            pltpu.VMEM((slots, 1), jnp.float32),
            pltpu.VMEM((slots, ff), jnp.bfloat16),
        ],
        compiler_params=pltpu.CompilerParams(
            dimension_semantics=("arbitrary",), vmem_limit_bytes=32 * 1024 * 1024
        ),
        cost_estimate=pl.CostEstimate(
            flops=6 * slots * total_width * ff,
            bytes_accessed=6 * total_width * ff + 8 * slots * half,
            transcendentals=slots * ff,
        ),
        name=f"expert_{piece}",
    )(core, own, other, gain[None, :], gate_weight, up_weight, down_weight)


def combine_kernel(routes_ref, weights_ref, *refs, capacity, pieces, experts):
    piece_refs, out_ref = refs[:pieces], refs[pieces]
    levels, rows, width = out_ref.shape
    picks = routes_ref.shape[1]
    wide = max(experts, 128)
    expert = lax.broadcasted_iota(jnp.int32, (rows, wide), 1)
    named = jnp.zeros((rows, wide), jnp.bool_)
    for pick in range(picks):
        named = named | (routes_ref[:, pick : pick + 1] == expert)
    earlier = (
        lax.broadcasted_iota(jnp.int32, (rows, rows), 1)
        < lax.broadcasted_iota(jnp.int32, (rows, rows), 0)
    ).astype(jnp.float32)
    rank = jnp.dot(
        earlier.astype(jnp.bfloat16),
        named.astype(jnp.float32).astype(jnp.bfloat16),
        preferred_element_type=jnp.float32,
    )
    slots = (experts // pieces) * capacity
    slot = lax.broadcasted_iota(jnp.int32, (rows, slots), 1)
    chosen = []
    for pick in range(picks):
        route = routes_ref[:, pick : pick + 1]
        mine = jnp.sum(jnp.where(expert == route, rank, 0.0), axis=1, keepdims=True)
        target = lax.div(route, pieces) * capacity + mine.astype(jnp.int32)
        for piece in range(pieces):
            here = jnp.where(lax.rem(route, pieces) == piece, target, -1)
            chosen.append((slot == here).astype(jnp.float32).astype(jnp.bfloat16))
    for level in range(levels):
        columns = slice(level * width, (level + 1) * width)
        total = jnp.zeros((rows, width), jnp.float32)
        for pick in range(picks):
            picked = jnp.zeros((rows, width), jnp.float32)
            for piece in range(pieces):
                picked += jnp.dot(
                    chosen[pick * pieces + piece],
                    piece_refs[piece][:, columns],
                    preferred_element_type=jnp.float32,
                )
            total += picked * weights_ref[:, pick : pick + 1]
        out_ref[level] = total.astype(jnp.bfloat16)


def combine(routes, route_weights, returned, capacity, levels, experts):
    rows, picks = routes.shape
    pieces = len(returned)
    slots, half = returned[0].shape
    return pl.pallas_call(
        functools.partial(combine_kernel, capacity=capacity, pieces=pieces, experts=experts),
        out_shape=jax.ShapeDtypeStruct((levels, rows, half // levels), jnp.bfloat16),
        in_specs=[whole()] * (2 + pieces),
        out_specs=whole(),
        cost_estimate=pl.CostEstimate(
            flops=2 * picks * pieces * slots * rows * half,
            bytes_accessed=2 * pieces * slots * half + 2 * rows * half,
            transcendentals=0,
        ),
        name="combine",
    )(routes, route_weights, *returned)


def shards(
    queries, keys, values, mix_weight, sub_gain, tokens, routes, route_weights,
    expert_gain, gate_weight, up_weight, down_weight,
):
    rows2, width = tokens.shape
    picks = routes.shape[1]
    groups, levels = lax.axis_size("ep"), lax.axis_size("tp") // CORES
    pieces = gate_weight.shape[0]
    experts = groups * pieces
    capacity = 3 * rows2 * picks // (2 * experts)

    by_level = exchange_levels(jnp.broadcast_to(tokens[None], (levels, rows2, width)))
    bundle = exchange_groups(attend_pack(queries, keys, values))
    outgoing = dispatch(routes, by_level, capacity, pieces, experts)
    slots, half = outgoing[0].shape
    layout = (groups, slots // groups, half)
    arrived = [exchange_groups(value.reshape(layout)).reshape(slots, half) for value in outgoing]
    attended = attend_compute(bundle, mix_weight, sub_gain, queries.shape[0])
    attended = exchange_groups(attended)
    returned = []
    for piece in range(pieces):
        own = arrived[piece]
        other = swap_core(own)
        kept, sent = run_expert(
            piece, own, other, expert_gain, gate_weight, up_weight, down_weight, width
        )
        partner = swap_core(sent)
        total = (kept.astype(jnp.float32) + partner.astype(jnp.float32)).astype(jnp.bfloat16)
        returned.append(exchange_groups(total.reshape(layout)).reshape(slots, half))
    combined = combine(routes, route_weights, returned, capacity, levels, experts)
    parts = exchange_levels(combined)
    moe_out = jnp.sum(parts.astype(jnp.float32), axis=0).astype(jnp.bfloat16)
    attn_out = attend_unpack(attended, queries.shape[1])
    return (attn_out, moe_out)


def solution(mesh):
    return jax.shard_map(
        shards,
        mesh=mesh,
        in_specs=(
            P("ep", "tp", None),
            P("ep", "tp", None),
            P("ep", "tp", None),
            P("tp"),
            P(),
            P("ep", "tp"),
            P("ep", None),
            P("ep", None),
            P(),
            P("ep", None, "tp"),
            P("ep", None, "tp"),
            P("ep", "tp", None),
        ),
        out_specs=(P("ep", "tp", None), P("ep", "tp")),
        check_vma=False,
    )
```

```python
import functools

import jax
import jax.numpy as jnp
from jax import lax
from jax.experimental import pallas as pl
from jax.experimental.pallas import tpu as pltpu
from jax.sharding import PartitionSpec as P


NEG_FILL = -1e30
SUB_EPS = 1e-05
NORM_EPS = 1e-06
CLAMP_LIMIT = 7.0
GLU_ALPHA = 1.702
OUT_SCALE = 0.8
LOG2E = 1.4426950408889634
CORES = 2
BF16 = jnp.bfloat16
F32 = jnp.float32


def whole():
    return pl.BlockSpec(memory_space=pltpu.VMEM)


def far():
    return pl.BlockSpec(memory_space=pl.ANY)


def weights():
    return pl.BlockSpec(memory_space=pltpu.HBM)


def scalars():
    return pl.BlockSpec(memory_space=pltpu.SMEM)


def shape_of(*sizes, dtype=BF16):
    return jax.ShapeDtypeStruct(sizes, dtype)


def grant(mebibytes, groups=4):
    size = min(60, mebibytes * max(1, groups // 4))
    return pltpu.CompilerParams(vmem_limit_bytes=size * 1024 * 1024)


def cost(flops, data, transcendentals=0):
    return pl.CostEstimate(
        flops=int(flops), bytes_accessed=int(data), transcendentals=int(transcendentals)
    )


def flip(value, axis, mask):
    pairs = [(source, source ^ mask) for source in range(lax.axis_size(axis))]
    return lax.ppermute(value, axis, pairs)


def levels_flip(value, mask):
    return flip(value, "tp", CORES * mask)


def cores_flip(value):
    return flip(value, "tp", 1)


def exchange(values):
    out = [values[0]]
    for mask in range(1, len(values)):
        out.append(flip(values[mask], "ep", mask))
    return out


def share_at(part, block, splits):
    return jnp.where(block % 2 == 0, part, splits - 1 - part)


def pack_kernel(place_ref, queries_ref, keys_ref, values_ref, *out_refs):
    place = place_ref[0]
    heads, rows, _ = keys_ref.shape
    splits = len(out_refs) // heads
    share = rows // splits
    for mask, out_ref in enumerate(out_refs):
        target = jnp.bitwise_xor(place, mask)
        head = lax.div(target, splits)
        start = share_at(lax.rem(target, splits), place, splits) * share
        out_ref[:rows] = keys_ref[head]
        out_ref[rows : 2 * rows] = values_ref[head]
        out_ref[2 * rows :] = queries_ref[head, pl.ds(pl.multiple_of(start, share), share)]


def pack(place, queries, keys, values, groups):
    rows, heads, width = queries.shape
    tall = 2 * rows + rows * heads // groups
    return pl.pallas_call(
        pack_kernel,
        out_shape=[shape_of(tall, width)] * groups,
        in_specs=[scalars(), whole(), whole(), whole()],
        out_specs=[whole()] * groups,
        cost_estimate=cost(2**21, 2 * groups * tall * width),
        compiler_params=grant(8),
        name="pack",
    )(place, *[jnp.transpose(value, (1, 0, 2)) for value in (queries, keys, values)])


def attention_kernel(place_ref, mix_ref, *refs, groups, rows, heads, scale):
    bundle_refs, gain_ref = refs[:groups], refs[groups]
    out_refs = refs[groups + 1 : 2 * groups + 1]
    bundle, outputs, scores, arrivals = refs[2 * groups + 1 :]
    place = place_ref[0]
    copies = []
    for mask in range(groups):
        copies.append(
            pltpu.make_async_copy(
                bundle_refs[mask], bundle.at[jnp.bitwise_xor(place, mask)], arrivals.at[mask]
            )
        )
    for copy in copies:
        copy.start()
    share, width = out_refs[0].shape
    splits = groups // heads
    mix = mix_ref[lax.div(place, splits)]
    part = lax.rem(place, splits)
    half = width // 2
    lane = lax.broadcasted_iota(jnp.int32, (share, width), 1)
    row = lax.broadcasted_iota(jnp.int32, (share, rows), 0)
    column = lax.broadcasted_iota(jnp.int32, (share, rows), 1)
    contract = (((1,), (1,)), ((), ()))
    factor = scale * LOG2E
    for copy in copies:
        copy.wait()
    for block in range(groups):
        visible = column <= row + (part if block % 2 == 0 else splits - 1 - part) * share
        queries = bundle[block, 2 * rows :, :]
        sums = []
        for side in range(2):
            own = (lane < half) if side == 0 else (lane >= half)
            query = jnp.where(own, queries, jnp.zeros_like(queries))
            top = jnp.full((share, 1), NEG_FILL, F32)
            for other in range(block + 1):
                score = lax.dot_general(
                    query, bundle[other, :rows, :], contract, preferred_element_type=F32
                )
                if other == block:
                    score = jnp.where(visible, score, NEG_FILL)
                scores[side, :, other * rows : (other + 1) * rows] = score
                top = jnp.maximum(top, jnp.max(score, axis=-1, keepdims=True))
            total = jnp.zeros((share, 1), F32)
            weighted = jnp.zeros((share, width), F32)
            for other in range(block + 1):
                score = scores[side, :, other * rows : (other + 1) * rows]
                weight = jnp.exp2((score - top) * factor)
                total += jnp.sum(weight, axis=-1, keepdims=True)
                weighted += jnp.dot(
                    weight.astype(BF16),
                    bundle[other, rows : 2 * rows, :],
                    preferred_element_type=F32,
                )
            sums.append(weighted / total)
        blend = sums[0] - mix * sums[1]
        mean = jnp.mean(blend * blend, axis=-1, keepdims=True)
        scaled = blend * lax.rsqrt(mean + SUB_EPS)
        outputs[block] = (scaled * gain_ref[...] * OUT_SCALE).astype(BF16)
    for mask in range(groups):
        out_refs[mask][...] = outputs[jnp.bitwise_xor(place, mask)]


def attention(place, bundles, mix_weight, sub_gain, rows):
    groups, heads = len(bundles), mix_weight.shape[0]
    tall, width = bundles[0].shape
    share = tall - 2 * rows
    pairs = groups * (groups + 1) // 2 * share * rows * 2
    return pl.pallas_call(
        functools.partial(
            attention_kernel, groups=groups, rows=rows, heads=heads, scale=(width // 2) ** -0.5
        ),
        out_shape=[shape_of(share, width)] * groups,
        in_specs=[scalars(), scalars()] + [far()] * groups + [whole()],
        out_specs=[whole()] * groups,
        scratch_shapes=[
            pltpu.VMEM((groups, tall, width), BF16),
            pltpu.VMEM((groups, share, width), BF16),
            pltpu.VMEM((2, share, groups * rows), F32),
            pltpu.SemaphoreType.DMA((groups,)),
        ],
        cost_estimate=cost(pairs * 4 * width, 2 * groups * tall * width, pairs),
        compiler_params=grant(16, groups),
        name="attention",
    )(place, mix_weight, *bundles, sub_gain[None, :])


def unpack_kernel(place_ref, *refs):
    part_refs, out_ref = refs[:-1], refs[-1]
    place = place_ref[0]
    groups, share = len(part_refs), part_refs[0].shape[0]
    splits = groups // out_ref.shape[0]
    for mask, ref in enumerate(part_refs):
        source = jnp.bitwise_xor(place, mask)
        start = share_at(lax.rem(source, splits), place, splits) * share
        out_ref[lax.div(source, splits), pl.ds(pl.multiple_of(start, share), share)] = ref[...]


def unpack(place, parts, heads):
    groups = len(parts)
    share, width = parts[0].shape
    rows = share * groups // heads
    by_head = pl.pallas_call(
        unpack_kernel,
        out_shape=shape_of(heads, rows, width),
        in_specs=[scalars()] + [whole()] * groups,
        out_specs=whole(),
        cost_estimate=cost(2**20, 4 * heads * rows * width),
        compiler_params=grant(4),
        name="unpack",
    )(place, *parts)
    return jnp.transpose(by_head, (1, 0, 2))


def ranks(named, strictly, axis):
    table = named.astype(F32).astype(BF16)
    earlier = strictly.astype(F32).astype(BF16)
    pair = (table, earlier) if axis == 1 else (earlier, table)
    return jnp.dot(*pair, preferred_element_type=F32)


def dispatch_kernel(place_ref, routes_ref, *refs, capacity, pieces, experts, groups):
    level_refs, out_refs = refs[:-groups], refs[-groups:]
    place = place_ref[0]
    rows, width = level_refs[0].shape
    picks = routes_ref.shape[0]
    tall = max(experts, 16)
    expert = lax.broadcasted_iota(jnp.int32, (tall, rows), 0)
    named = jnp.zeros((tall, rows), jnp.bool_)
    for pick in range(picks):
        named = named | (routes_ref[pick : pick + 1, :] == expert)
    first = lax.broadcasted_iota(jnp.int32, (rows, rows), 0)
    second = lax.broadcasted_iota(jnp.int32, (rows, rows), 1)
    rank = ranks(named, first < second, 1)
    targets = []
    for pick in range(picks):
        route = routes_ref[pick : pick + 1, :]
        mine = jnp.sum(jnp.where(expert == route, rank, 0.0), axis=0, keepdims=True)
        targets.append(route * capacity + mine.astype(jnp.int32))
    slots = pieces * capacity
    slot = lax.broadcasted_iota(jnp.int32, (slots, rows), 0)
    for mask in range(groups):
        here = slot + jnp.bitwise_xor(place, mask) * slots
        chosen = jnp.zeros((slots, rows), jnp.bool_)
        for pick in range(picks):
            chosen = chosen | (here == targets[pick])
        onehot = chosen.astype(F32).astype(BF16)
        for level, ref in enumerate(level_refs):
            out_refs[mask][:, level * width : (level + 1) * width] = jnp.dot(
                onehot, ref[...], preferred_element_type=F32
            ).astype(BF16)


def dispatch(place, routes, by_level, capacity, pieces, experts, groups):
    rows, width = by_level[0].shape
    slots, wide = pieces * capacity, len(by_level) * width
    return pl.pallas_call(
        functools.partial(
            dispatch_kernel, capacity=capacity, pieces=pieces, experts=experts, groups=groups
        ),
        out_shape=[shape_of(slots, wide)] * groups,
        in_specs=[scalars(), whole()] + [whole()] * len(by_level),
        out_specs=[whole()] * groups,
        cost_estimate=cost(2 * groups * slots * rows * wide, 4 * groups * slots * wide),
        compiler_params=grant(8),
        name="dispatch",
    )(place, routes.T, *by_level)


def block_start(spot_ref, level, side, width):
    core = spot_ref[2] if side == 0 else 1 - spot_ref[2]
    return (CORES * jnp.bitwise_xor(spot_ref[1], level) + core) * width


def hidden_kernel(spot_ref, *refs, count, groups, capacity, width):
    slot_refs, (gain_ref, gate_hbm, up_hbm, hidden_ref) = refs[:count], refs[count : count + 4]
    normed, gate_vmem, up_vmem, arrivals = refs[count + 4 :]
    pieces, total_width, _ = gate_hbm.shape
    tile = gate_vmem.shape[2]
    steps = gate_vmem.shape[0] // pieces
    chunks = count // groups // 2
    span = slot_refs[0].shape[1] // width
    copies = []
    for index in range(pieces * steps):
        columns = pl.ds(index % steps * tile, tile)
        for kind, (source, target) in enumerate(((gate_hbm, gate_vmem), (up_hbm, up_vmem))):
            copies.append(
                pltpu.make_async_copy(
                    source.at[index // steps, :, columns],
                    target.at[index],
                    arrivals.at[2 * index + kind],
                )
            )
    for copy in copies:
        copy.start()
    factors = [[None] * groups for _ in range(pieces)]
    for group in range(groups):
        squares = jnp.zeros((pieces * capacity, 1), F32)
        for side in range(CORES):
            for chunk in range(chunks):
                ref = slot_refs[(side * chunks + chunk) * groups + group]
                for inner in range(span):
                    floats = ref[:, inner * width : (inner + 1) * width].astype(F32)
                    squares += jnp.sum(floats * floats, axis=-1, keepdims=True)
                    start = block_start(spot_ref, chunk * span + inner, side, width)
                    place = pl.ds(pl.multiple_of(start, width), width)
                    value = (floats * gain_ref[:, place]).astype(BF16)
                    for piece in range(pieces):
                        normed[piece, group * capacity : (group + 1) * capacity, place] = value[
                            piece * capacity : (piece + 1) * capacity
                        ]
        factor = lax.rsqrt(squares / total_width + NORM_EPS)
        for piece in range(pieces):
            factors[piece][group] = factor[piece * capacity : (piece + 1) * capacity]
    for piece in range(pieces):
        factor = jnp.concatenate(factors[piece], axis=0)
        for step in range(steps):
            index = piece * steps + step
            copies[2 * index].wait()
            gate = jnp.dot(normed[piece], gate_vmem[index], preferred_element_type=F32)
            copies[2 * index + 1].wait()
            up = jnp.dot(normed[piece], up_vmem[index], preferred_element_type=F32)
            gate = jnp.minimum(gate * factor, CLAMP_LIMIT)
            up = jnp.clip(up * factor, -CLAMP_LIMIT, CLAMP_LIMIT)
            hidden_ref[piece, :, step * tile : (step + 1) * tile] = (
                (up + 1.0) * gate * jax.nn.sigmoid(GLU_ALPHA * gate)
            ).astype(BF16)


def hidden_units(spot, own, other, gain, gate_weight, up_weight, groups, capacity, width):
    pieces, total_width, ff = gate_weight.shape
    tile = 256 if ff % 256 == 0 else ff
    steps = ff // tile
    tables = [table for side in (own, other) for chunk in side for table in chunk]
    rows = groups * capacity
    return pl.pallas_call(
        functools.partial(
            hidden_kernel, count=len(tables), groups=groups, capacity=capacity, width=width
        ),
        out_shape=shape_of(pieces, rows, ff),
        in_specs=[scalars()] + [whole()] * (len(tables) + 1) + [weights()] * 2,
        out_specs=whole(),
        scratch_shapes=[
            pltpu.VMEM((pieces, rows, total_width), BF16),
            pltpu.VMEM((pieces * steps, total_width, tile), BF16),
            pltpu.VMEM((pieces * steps, total_width, tile), BF16),
            pltpu.SemaphoreType.DMA((2 * pieces * steps,)),
        ],
        cost_estimate=cost(
            4 * pieces * rows * total_width * ff,
            4 * pieces * total_width * (ff + rows),
            pieces * rows * ff,
        ),
        compiler_params=grant(24),
        name="hidden",
    )(spot, *tables, gain[None, :], gate_weight, up_weight)


def down_kernel(
    spot_ref, hidden_ref, down_hbm, sent_ref, kept_ref, down_vmem, arrivals,
    *, groups, capacity, width, start,
):
    pieces = hidden_ref.shape[0]
    part = sent_ref.shape[1]
    copies = []
    blocks = arrivals.shape[0] // (pieces * CORES)
    piece_width = part // blocks
    for side in (1, 0):
        for piece in range(pieces):
            for level in range(blocks):
                offset = block_start(spot_ref, level, side, width) + start
                index = (side * pieces + piece) * blocks + level
                copies.append(
                    pltpu.make_async_copy(
                        down_hbm.at[
                            piece, :, pl.ds(pl.multiple_of(offset, piece_width), piece_width)
                        ],
                        down_vmem.at[
                            side * pieces + piece,
                            :,
                            pl.ds(level * piece_width, piece_width),
                        ],
                        arrivals.at[index],
                    )
                )
    for copy in copies:
        copy.start()
    taken = 0
    for side, ref in ((1, sent_ref), (0, kept_ref)):
        for piece in range(pieces):
            for copy in copies[taken : taken + blocks]:
                copy.wait()
            taken += blocks
            value = jnp.dot(
                hidden_ref[piece],
                down_vmem[side * pieces + piece],
                preferred_element_type=F32,
            ).astype(BF16)
            for group in range(groups):
                row = (group * pieces + piece) * capacity
                ref[row : row + capacity] = value[group * capacity : (group + 1) * capacity]


def down(spot, hidden, down_weight, groups, capacity, width, levels, start, piece_width):
    pieces, rows, ff = hidden.shape
    part = levels * piece_width
    return pl.pallas_call(
        functools.partial(
            down_kernel, groups=groups, capacity=capacity, width=width, start=start
        ),
        out_shape=[shape_of(pieces * rows, part)] * 2,
        in_specs=[scalars(), whole(), weights()],
        out_specs=[whole()] * 2,
        scratch_shapes=[
            pltpu.VMEM((CORES * pieces, ff, part), BF16),
            pltpu.SemaphoreType.DMA((CORES * pieces * levels,)),
        ],
        cost_estimate=cost(
            2 * CORES * pieces * rows * ff * part, 2 * CORES * pieces * part * (ff + rows)
        ),
        compiler_params=grant(10),
        name="down",
    )(spot, hidden, down_weight)


def add_kernel(kept_ref, partner_ref, *out_refs):
    rows = out_refs[0].shape[0]
    for group, ref in enumerate(out_refs):
        place = slice(group * rows, (group + 1) * rows)
        ref[...] = (kept_ref[place].astype(F32) + partner_ref[place].astype(F32)).astype(BF16)


def add_cores(kept, partner, groups):
    rows, width = kept.shape
    return pl.pallas_call(
        add_kernel,
        out_shape=[shape_of(rows // groups, width)] * groups,
        in_specs=[whole()] * 2,
        out_specs=[whole()] * groups,
        cost_estimate=cost(2**21, 6 * rows * width),
        compiler_params=grant(6),
        name="add_cores",
    )(kept, partner)


def plan_kernel(place_ref, routes_ref, out_ref, *, capacity, pieces, experts):
    rows, picks = routes_ref.shape
    slots = out_ref.shape[2]
    groups = out_ref.shape[0] // picks
    wide = max(experts, 128)
    expert = lax.broadcasted_iota(jnp.int32, (rows, wide), 1)
    named = jnp.zeros((rows, wide), jnp.bool_)
    for pick in range(picks):
        named = named | (routes_ref[:, pick : pick + 1] == expert)
    first = lax.broadcasted_iota(jnp.int32, (rows, rows), 0)
    second = lax.broadcasted_iota(jnp.int32, (rows, rows), 1)
    rank = ranks(named, second < first, 0)
    slot = lax.broadcasted_iota(jnp.int32, (rows, slots), 1)
    for pick in range(picks):
        route = routes_ref[:, pick : pick + 1]
        mine = jnp.sum(jnp.where(expert == route, rank, 0.0), axis=1, keepdims=True)
        target = route * capacity + mine.astype(jnp.int32)
        for mask in range(groups):
            here = slot + jnp.bitwise_xor(place_ref[0], mask) * slots
            out_ref[pick * groups + mask] = (here == target).astype(F32).astype(BF16)


def plan(place, routes, capacity, pieces, experts, groups):
    rows, picks = routes.shape
    slots = pieces * capacity
    return pl.pallas_call(
        functools.partial(plan_kernel, capacity=capacity, pieces=pieces, experts=experts),
        out_shape=shape_of(picks * groups, rows, slots),
        in_specs=[scalars(), whole()],
        out_specs=whole(),
        cost_estimate=cost(2**25, 2 * picks * groups * rows * slots),
        compiler_params=grant(6),
        name="plan",
    )(place, routes)


def gather_kernel(chosen_ref, weights_ref, *refs, groups):
    table_refs, out_refs = refs[:groups], refs[groups:]
    picks = chosen_ref.shape[0] // groups
    width = out_refs[0].shape[1]
    total = None
    for pick in range(picks):
        picked = None
        for group in range(groups):
            part = jnp.dot(
                chosen_ref[pick * groups + group],
                table_refs[group][...],
                preferred_element_type=F32,
            )
            picked = part if picked is None else picked + part
        picked = picked * weights_ref[:, pick : pick + 1]
        total = picked if total is None else total + picked
    for level, ref in enumerate(out_refs):
        ref[...] = total[:, level * width : (level + 1) * width].astype(BF16)


def gather(chosen, route_weights, tables, levels):
    groups = len(tables)
    rows, picks = route_weights.shape
    slots, width = tables[0].shape
    return pl.pallas_call(
        functools.partial(gather_kernel, groups=groups),
        out_shape=[shape_of(rows, width // levels)] * levels,
        in_specs=[whole()] * (2 + groups),
        out_specs=[whole()] * levels,
        cost_estimate=cost(
            2 * picks * groups * slots * rows * width,
            2 * groups * slots * (width + picks * rows) + 2 * rows * width,
        ),
        compiler_params=grant(8),
        name="gather",
    )(chosen, route_weights, *tables)


def final_kernel(*refs, parts):
    out_ref = refs[-1]
    count = (len(refs) - 1) // parts
    width = out_ref.shape[1] // parts
    for part in range(parts):
        total = refs[part * count][...].astype(F32)
        for level in range(1, count):
            total += refs[part * count + level][...].astype(F32)
        out_ref[:, part * width : (part + 1) * width] = total.astype(BF16)


def final(parts):
    rows, width = parts[0][0].shape
    flat = [value for part in parts for value in part]
    return pl.pallas_call(
        functools.partial(final_kernel, parts=len(parts)),
        out_shape=shape_of(rows, width * len(parts)),
        in_specs=[whole()] * len(flat),
        out_specs=whole(),
        cost_estimate=cost(2**20, 2 * len(flat) * rows * width),
        compiler_params=grant(4),
        name="final",
    )(*flat)


def shards(
    queries, keys, values, mix_weight, sub_gain, tokens, routes, route_weights,
    expert_gain, gate_weight, up_weight, down_weight,
):
    rows2, width = tokens.shape
    picks = routes.shape[1]
    groups, levels = lax.axis_size("ep"), lax.axis_size("tp") // CORES
    pieces = gate_weight.shape[0]
    experts = groups * pieces
    capacity = 3 * rows2 * picks // (2 * experts)
    parts = parts_of(width)
    tp_index = lax.axis_index("tp")
    spot = jnp.stack([lax.axis_index("ep"), tp_index // CORES, tp_index % CORES])
    place = spot = spot.astype(jnp.int32)

    by_level = [tokens]
    for mask in range(1, levels):
        by_level.append(levels_flip(tokens, mask))
    bundles = pack(place, queries, keys, values, groups)
    bundles = exchange(bundles)
    chosen = plan(place, routes, capacity, pieces, experts, groups)
    own, other = [], []
    for chunk in range(2):
        some = by_level[chunk * levels // 2 : (chunk + 1) * levels // 2]
        tables = dispatch(place, routes, some, capacity, pieces, experts, groups)
        own.append(exchange(tables))
    for chunk in range(2):
        swapped = []
        for table in own[chunk]:
            swapped.append(cores_flip(table))
        other.append(swapped)
    hidden = hidden_units(
        spot, own, other, expert_gain, gate_weight, up_weight, groups, capacity, width
    )
    results = []
    for part in range(parts):
        sent, kept = down(
            spot, hidden, down_weight, groups, capacity, width, levels,
            part * (width // parts), width // parts,
        )
        partner = cores_flip(sent)
        tables = add_cores(kept, partner, groups)
        tables = exchange(tables)
        combined = gather(chosen, route_weights, tables, levels)
        arrived = [combined[0]]
        for mask in range(1, levels):
            arrived.append(levels_flip(combined[mask], mask))
        results.append(arrived)
    attended = attention(place, bundles, mix_weight, sub_gain, queries.shape[0])
    attended = exchange(attended)
    moe_out = final(results)
    attn_out = unpack(place, attended, queries.shape[1])
    return (attn_out, moe_out)


def parts_of(width):
    return 2 if width % 256 == 0 else 1


def solution(mesh):
    return jax.shard_map(
        shards,
        mesh=mesh,
        in_specs=(
            P("ep", "tp", None),
            P("ep", "tp", None),
            P("ep", "tp", None),
            P("tp"),
            P(),
            P("ep", "tp"),
            P("ep", None),
            P("ep", None),
            P(),
            P("ep", None, "tp"),
            P("ep", None, "tp"),
            P("ep", "tp", None),
        ),
        out_specs=(P("ep", "tp", None), P("ep", "tp")),
        check_vma=False,
    )
```

```python
import functools

import jax
import jax.numpy as jnp
from jax import lax
from jax.experimental import pallas as pl
from jax.experimental.pallas import tpu as pltpu
from jax.sharding import PartitionSpec as P


NEG_FILL = -1e30
SUB_EPS = 1e-05
NORM_EPS = 1e-06
CLAMP_LIMIT = 7.0
GLU_ALPHA = 1.702
OUT_SCALE = 0.8
LOG2E = 1.4426950408889634
CORES = 2
FETCH_GRANT = 44
BF16 = jnp.bfloat16
F32 = jnp.float32


def whole():
    return pl.BlockSpec(memory_space=pltpu.VMEM)


def far():
    return pl.BlockSpec(memory_space=pl.ANY)


def scalars():
    return pl.BlockSpec(memory_space=pltpu.SMEM)


def shape_of(*sizes, dtype=BF16):
    return jax.ShapeDtypeStruct(sizes, dtype)


def grant(mebibytes, groups=4):
    size = min(60, mebibytes * max(1, groups // 4))
    return pltpu.CompilerParams(vmem_limit_bytes=size * 1024 * 1024)


def cost(flops, data, transcendentals=0):
    return pl.CostEstimate(
        flops=int(flops), bytes_accessed=int(data), transcendentals=int(transcendentals)
    )


def flip(value, axis, mask):
    pairs = [(source, source ^ mask) for source in range(lax.axis_size(axis))]
    return lax.ppermute(value, axis, pairs)


def levels_flip(value, mask):
    return flip(value, "tp", CORES * mask)


def cores_flip(value):
    return flip(value, "tp", 1)


def exchange(values):
    out = [values[0]]
    for mask in range(1, len(values)):
        out.append(flip(values[mask], "ep", mask))
    return out


def share_at(part, block, splits):
    return jnp.where(block % 2 == 0, part, splits - 1 - part)


def pack_kernel(place_ref, queries_ref, keys_ref, values_ref, *out_refs):
    place = place_ref[0]
    heads, rows, _ = keys_ref.shape
    splits = len(out_refs) // heads
    share = rows // splits
    for mask, out_ref in enumerate(out_refs):
        target = jnp.bitwise_xor(place, mask)
        head = lax.div(target, splits)
        start = share_at(lax.rem(target, splits), place, splits) * share
        out_ref[:rows] = keys_ref[head]
        out_ref[rows : 2 * rows] = values_ref[head]
        out_ref[2 * rows :] = queries_ref[head, pl.ds(pl.multiple_of(start, share), share)]


def pack(place, queries, keys, values, groups):
    rows, heads, width = queries.shape
    tall = 2 * rows + rows * heads // groups
    return pl.pallas_call(
        pack_kernel,
        out_shape=[shape_of(tall, width)] * groups,
        in_specs=[scalars(), whole(), whole(), whole()],
        out_specs=[whole()] * groups,
        cost_estimate=cost(2**21, 2 * groups * tall * width),
        compiler_params=grant(8),
        name="pack",
    )(place, *[jnp.transpose(value, (1, 0, 2)) for value in (queries, keys, values)])


def attention_kernel(place_ref, mix_ref, *refs, groups, rows, heads, scale):
    bundle_refs, gain_ref = refs[:groups], refs[groups]
    out_refs = refs[groups + 1 : 2 * groups + 1]
    bundle, outputs, scores, arrivals = refs[2 * groups + 1 :]
    place = place_ref[0]
    copies = []
    for mask in range(groups):
        copies.append(
            pltpu.make_async_copy(
                bundle_refs[mask], bundle.at[jnp.bitwise_xor(place, mask)], arrivals.at[mask]
            )
        )
    for copy in copies:
        copy.start()
    share, width = out_refs[0].shape
    splits = groups // heads
    mix = mix_ref[lax.div(place, splits)]
    part = lax.rem(place, splits)
    half = width // 2
    lane = lax.broadcasted_iota(jnp.int32, (share, width), 1)
    row = lax.broadcasted_iota(jnp.int32, (share, rows), 0)
    column = lax.broadcasted_iota(jnp.int32, (share, rows), 1)
    contract = (((1,), (1,)), ((), ()))
    factor = scale * LOG2E
    for copy in copies:
        copy.wait()
    tops = [None, None]
    for block in range(groups):
        visible = column <= row + (part if block % 2 == 0 else splits - 1 - part) * share
        queries = bundle[block, 2 * rows :, :]
        empty = jnp.zeros_like(queries)
        for side in range(2):
            query = jnp.where((lane < half) if side == 0 else (lane >= half), queries, empty)
            top = jnp.full((share, width), NEG_FILL, F32)
            for other in range(block + 1):
                score = lax.dot_general(
                    query, bundle[other, :rows, :], contract, preferred_element_type=F32
                )
                if other == block:
                    score = jnp.where(visible, score, NEG_FILL)
                scores[side, :, other * rows : (other + 1) * rows] = score
                for start in range(0, rows, width):
                    top = jnp.maximum(top, score[:, start : start + width])
            tops[side] = jnp.max(top, axis=-1, keepdims=True)
        sums = []
        for side in range(2):
            top = tops[side]
            total = jnp.zeros((share, width), F32)
            weighted = jnp.zeros((share, width), F32)
            for other in range(block + 1):
                score = scores[side, :, other * rows : (other + 1) * rows]
                weight = jnp.exp2((score - top) * factor)
                for start in range(0, rows, width):
                    total += weight[:, start : start + width]
                weighted += jnp.dot(
                    weight.astype(BF16),
                    bundle[other, rows : 2 * rows, :],
                    preferred_element_type=F32,
                )
            sums.append(weighted / jnp.sum(total, axis=-1, keepdims=True))
        blend = sums[0] - mix * sums[1]
        mean = jnp.mean(blend * blend, axis=-1, keepdims=True)
        scaled = blend * lax.rsqrt(mean + SUB_EPS)
        outputs[block] = (scaled * gain_ref[...] * OUT_SCALE).astype(BF16)
    for mask in range(groups):
        out_refs[mask][...] = outputs[jnp.bitwise_xor(place, mask)]


def attention(place, bundles, mix_weight, sub_gain, rows):
    groups, heads = len(bundles), mix_weight.shape[0]
    tall, width = bundles[0].shape
    share = tall - 2 * rows
    pairs = groups * (groups + 1) // 2 * share * rows * 2
    return pl.pallas_call(
        functools.partial(
            attention_kernel, groups=groups, rows=rows, heads=heads, scale=(width // 2) ** -0.5
        ),
        out_shape=[shape_of(share, width)] * groups,
        in_specs=[scalars(), scalars()] + [far()] * groups + [whole()],
        out_specs=[whole()] * groups,
        scratch_shapes=[
            pltpu.VMEM((groups, tall, width), BF16),
            pltpu.VMEM((groups, share, width), BF16),
            pltpu.VMEM((2, share, groups * rows), F32),
            pltpu.SemaphoreType.DMA((groups,)),
        ],
        cost_estimate=cost(pairs * 4 * width, 2 * groups * tall * width, pairs),
        compiler_params=grant(16, groups),
        name="attention",
    )(place, mix_weight, *bundles, sub_gain[None, :])


def unpack_kernel(place_ref, *refs):
    part_refs, out_ref = refs[:-1], refs[-1]
    place = place_ref[0]
    groups, share = len(part_refs), part_refs[0].shape[0]
    splits = groups // out_ref.shape[0]
    for mask, ref in enumerate(part_refs):
        source = jnp.bitwise_xor(place, mask)
        start = share_at(lax.rem(source, splits), place, splits) * share
        out_ref[lax.div(source, splits), pl.ds(pl.multiple_of(start, share), share)] = ref[...]


def unpack(place, parts, heads):
    groups = len(parts)
    share, width = parts[0].shape
    rows = share * groups // heads
    by_head = pl.pallas_call(
        unpack_kernel,
        out_shape=shape_of(heads, rows, width),
        in_specs=[scalars()] + [whole()] * groups,
        out_specs=whole(),
        cost_estimate=cost(2**20, 4 * heads * rows * width),
        compiler_params=grant(4),
        name="unpack",
    )(place, *parts)
    return jnp.transpose(by_head, (1, 0, 2))


def ranks(named, strictly, axis):
    table = named.astype(F32).astype(BF16)
    earlier = strictly.astype(F32).astype(BF16)
    pair = (table, earlier) if axis == 1 else (earlier, table)
    return jnp.dot(*pair, preferred_element_type=F32)


def dispatch_kernel(place_ref, routes_ref, *refs, capacity, pieces, experts, groups):
    level_refs, out_refs = refs[:-groups], refs[-groups:]
    place = place_ref[0]
    rows, width = level_refs[0].shape
    picks = routes_ref.shape[0]
    tall = max(experts, 16)
    expert = lax.broadcasted_iota(jnp.int32, (tall, rows), 0)
    named = jnp.zeros((tall, rows), jnp.bool_)
    for pick in range(picks):
        named = named | (routes_ref[pick : pick + 1, :] == expert)
    first = lax.broadcasted_iota(jnp.int32, (rows, rows), 0)
    second = lax.broadcasted_iota(jnp.int32, (rows, rows), 1)
    rank = ranks(named, first < second, 1)
    targets = []
    for pick in range(picks):
        route = routes_ref[pick : pick + 1, :]
        mine = jnp.sum(jnp.where(expert == route, rank, 0.0), axis=0, keepdims=True)
        targets.append(route * capacity + mine.astype(jnp.int32))
    slots = pieces * capacity
    slot = lax.broadcasted_iota(jnp.int32, (slots, rows), 0)
    for mask in range(groups):
        here = slot + jnp.bitwise_xor(place, mask) * slots
        chosen = jnp.zeros((slots, rows), jnp.bool_)
        for pick in range(picks):
            chosen = chosen | (here == targets[pick])
        onehot = chosen.astype(F32).astype(BF16)
        for level, ref in enumerate(level_refs):
            out_refs[mask][:, level * width : (level + 1) * width] = jnp.dot(
                onehot, ref[...], preferred_element_type=F32
            ).astype(BF16)


def dispatch(place, routes, by_level, capacity, pieces, experts, groups):
    rows, width = by_level[0].shape
    slots, wide = pieces * capacity, len(by_level) * width
    return pl.pallas_call(
        functools.partial(
            dispatch_kernel, capacity=capacity, pieces=pieces, experts=experts, groups=groups
        ),
        out_shape=[shape_of(slots, wide)] * groups,
        in_specs=[scalars(), whole()] + [whole()] * len(by_level),
        out_specs=[whole()] * groups,
        cost_estimate=cost(2 * groups * slots * rows * wide, 4 * groups * slots * wide),
        compiler_params=grant(8),
        name="dispatch",
    )(place, routes, *by_level)


def block_start(spot_ref, level, side, width):
    core = spot_ref[2] if side == 0 else 1 - spot_ref[2]
    return (CORES * jnp.bitwise_xor(spot_ref[1], level) + core) * width


def fetch_kernel(*refs):
    count = (len(refs) - 1) // 2
    arrivals = refs[-1]
    copies = []
    for source, target in zip(refs[:count], refs[count : 2 * count]):
        parts = [()] if len(source.shape) < 3 else [(piece,) for piece in range(source.shape[0])]
        for part in parts:
            copies.append(
                pltpu.make_async_copy(source.at[part], target.at[part], arrivals.at[len(copies)])
            )
    for copy in copies:
        copy.start()
    for copy in copies:
        copy.wait()


def fetch(*arrays, mebibytes):
    return pl.pallas_call(
        fetch_kernel,
        out_shape=[shape_of(*array.shape, dtype=array.dtype) for array in arrays],
        in_specs=[far()] * len(arrays),
        out_specs=[whole()] * len(arrays),
        scratch_shapes=[pltpu.SemaphoreType.DMA((2 * len(arrays),))],
        cost_estimate=cost(2**20, sum(4 * array.size for array in arrays)),
        compiler_params=grant(mebibytes),
    )(*arrays)


def hidden_kernel(spot_ref, *refs, count, groups, capacity, width):
    slot_refs = refs[:count]
    gain_ref, gate_ref, up_ref, hidden_ref, normed = refs[count:]
    pieces, total_width, ff = gate_ref.shape
    tile = 256 if ff % 256 == 0 else ff
    chunks = count // groups // 2
    span = slot_refs[0].shape[1] // width
    factors = [[None] * groups for _ in range(pieces)]
    for group in range(groups):
        squares = jnp.zeros((pieces * capacity, 1), F32)
        for side in range(CORES):
            for chunk in range(chunks):
                ref = slot_refs[(side * chunks + chunk) * groups + group]
                for inner in range(span):
                    floats = ref[:, inner * width : (inner + 1) * width].astype(F32)
                    squares += jnp.sum(floats * floats, axis=-1, keepdims=True)
                    start = block_start(spot_ref, chunk * span + inner, side, width)
                    place = pl.ds(pl.multiple_of(start, width), width)
                    value = (floats * gain_ref[:, place]).astype(BF16)
                    for piece in range(pieces):
                        normed[piece, group * capacity : (group + 1) * capacity, place] = value[
                            piece * capacity : (piece + 1) * capacity
                        ]
        factor = lax.rsqrt(squares / total_width + NORM_EPS)
        for piece in range(pieces):
            factors[piece][group] = factor[piece * capacity : (piece + 1) * capacity]
    for piece in range(pieces):
        factor = jnp.concatenate(factors[piece], axis=0)
        for start in range(0, ff, tile):
            columns = slice(start, start + tile)
            gate = jnp.dot(normed[piece], gate_ref[piece, :, columns], preferred_element_type=F32)
            up = jnp.dot(normed[piece], up_ref[piece, :, columns], preferred_element_type=F32)
            gate = jnp.minimum(gate * factor, CLAMP_LIMIT)
            up = jnp.clip(up * factor, -CLAMP_LIMIT, CLAMP_LIMIT)
            hidden_ref[piece, :, columns] = (
                (up + 1.0) * gate * jax.nn.sigmoid(GLU_ALPHA * gate)
            ).astype(BF16)


def hidden_units(spot, own, other, gain, gate_weight, up_weight, groups, capacity, width):
    pieces, total_width, ff = gate_weight.shape
    tables = [table for side in (own, other) for chunk in side for table in chunk]
    rows = groups * capacity
    return pl.pallas_call(
        functools.partial(
            hidden_kernel, count=len(tables), groups=groups, capacity=capacity, width=width
        ),
        out_shape=shape_of(pieces, rows, ff),
        in_specs=[scalars()] + [whole()] * (len(tables) + 3),
        out_specs=whole(),
        scratch_shapes=[pltpu.VMEM((pieces, rows, total_width), BF16)],
        cost_estimate=cost(
            4 * pieces * rows * total_width * ff,
            4 * pieces * total_width * (ff + rows),
            pieces * rows * ff,
        ),
        compiler_params=grant(20),
        name="hidden",
    )(spot, *tables, gain[None, :], gate_weight, up_weight)


def down_kernel(
    spot_ref, hidden_ref, down_ref, sent_ref, kept_ref, *, groups, capacity, width, first
):
    pieces = hidden_ref.shape[0]
    for side, ref in ((1, sent_ref), (0, kept_ref)):
        for piece in range(pieces):
            for inner in range(ref.shape[1] // width):
                start = block_start(spot_ref, first + inner, side, width)
                value = jnp.dot(
                    hidden_ref[piece],
                    down_ref[piece, :, pl.ds(pl.multiple_of(start, width), width)],
                    preferred_element_type=F32,
                ).astype(BF16)
                for group in range(groups):
                    row = (group * pieces + piece) * capacity
                    ref[row : row + capacity, inner * width : (inner + 1) * width] = value[
                        group * capacity : (group + 1) * capacity
                    ]


def down(spot, hidden, down_weight, groups, capacity, width, first, span):
    pieces, rows, ff = hidden.shape
    part = span * width
    return pl.pallas_call(
        functools.partial(down_kernel, groups=groups, capacity=capacity, width=width, first=first),
        out_shape=[shape_of(pieces * rows, part)] * 2,
        in_specs=[scalars(), whole(), whole()],
        out_specs=[whole()] * 2,
        cost_estimate=cost(
            2 * CORES * pieces * rows * ff * part, 2 * CORES * pieces * part * (ff + rows)
        ),
        compiler_params=grant(12),
        name="down",
    )(spot, hidden, down_weight)


def add_kernel(kept_ref, partner_ref, *out_refs):
    rows = out_refs[0].shape[0]
    for group, ref in enumerate(out_refs):
        place = slice(group * rows, (group + 1) * rows)
        ref[...] = (kept_ref[place].astype(F32) + partner_ref[place].astype(F32)).astype(BF16)


def add_cores(kept, partner, groups):
    rows, width = kept.shape
    return pl.pallas_call(
        add_kernel,
        out_shape=[shape_of(rows // groups, width)] * groups,
        in_specs=[whole()] * 2,
        out_specs=[whole()] * groups,
        cost_estimate=cost(2**21, 6 * rows * width),
        compiler_params=grant(6),
        name="add_cores",
    )(kept, partner)


def part_kernel(kept_ref, partner_ref, mine_ref, *out_refs):
    width = mine_ref.shape[1]
    for level, ref in enumerate((mine_ref,) + out_refs):
        place = slice(level * width, (level + 1) * width)
        total = kept_ref[:, place].astype(F32) + partner_ref[:, place].astype(F32)
        ref[...] = total.astype(ref.dtype)


def part_levels(kept, partner, levels):
    rows, width = kept.shape
    own = width // levels
    return pl.pallas_call(
        part_kernel,
        out_shape=[shape_of(rows, own, dtype=F32)] + [shape_of(rows, own)] * (levels - 1),
        in_specs=[whole()] * 2,
        out_specs=[whole()] * levels,
        cost_estimate=cost(2**21, 6 * rows * width),
        compiler_params=grant(6),
        name="part_levels",
    )(kept, partner)


def sum_kernel(*refs, groups):
    value_refs, out_refs = refs[:-groups], refs[-groups:]
    rows = out_refs[0].shape[0]
    for group, ref in enumerate(out_refs):
        place = slice(group * rows, (group + 1) * rows)
        total = value_refs[0][place]
        for value_ref in value_refs[1:]:
            total += value_ref[place].astype(F32)
        ref[...] = total.astype(BF16)


def sum_levels(values, groups):
    rows, width = values[0].shape
    return pl.pallas_call(
        functools.partial(sum_kernel, groups=groups),
        out_shape=[shape_of(rows // groups, width)] * groups,
        in_specs=[whole()] * len(values),
        out_specs=[whole()] * groups,
        cost_estimate=cost(2**21, 6 * rows * width),
        compiler_params=grant(6),
        name="sum_levels",
    )(*values)


def plan_kernel(
    place_ref, routes_ref, weights_ref, out_ref, scale_ref, *, capacity, pieces, experts
):
    picks, rows = routes_ref.shape
    slots = out_ref.shape[2]
    groups = out_ref.shape[0] // picks
    wide = max(experts, 128)
    first = lax.broadcasted_iota(jnp.int32, (rows, rows), 0)
    second = lax.broadcasted_iota(jnp.int32, (rows, rows), 1)

    def column(row):
        return jnp.sum(jnp.where(first == second, row, 0.0), axis=1, keepdims=True)

    expert = lax.broadcasted_iota(jnp.int32, (rows, wide), 1)
    named = jnp.zeros((rows, wide), jnp.bool_)
    scale = jnp.zeros((rows, scale_ref.shape[1]), F32)
    lane = lax.broadcasted_iota(jnp.int32, scale.shape, 1)
    routes = []
    for pick in range(picks):
        routes.append(column(routes_ref[pick : pick + 1, :].astype(F32)).astype(jnp.int32))
        named = named | (routes[pick] == expert)
        scale = jnp.where(lane == pick, column(weights_ref[pick : pick + 1, :]), scale)
    scale_ref[...] = scale
    rank = ranks(named, second < first, 0)
    slot = lax.broadcasted_iota(jnp.int32, (rows, slots), 1)
    for pick in range(picks):
        mine = jnp.sum(jnp.where(expert == routes[pick], rank, 0.0), axis=1, keepdims=True)
        target = routes[pick] * capacity + mine.astype(jnp.int32)
        for mask in range(groups):
            here = slot + jnp.bitwise_xor(place_ref[0], mask) * slots
            out_ref[pick * groups + mask] = (here == target).astype(F32).astype(BF16)


def plan(place, routes, route_weights, capacity, pieces, experts, groups):
    picks, rows = routes.shape
    slots = pieces * capacity
    return pl.pallas_call(
        functools.partial(plan_kernel, capacity=capacity, pieces=pieces, experts=experts),
        out_shape=[shape_of(picks * groups, rows, slots), shape_of(rows, 128, dtype=F32)],
        in_specs=[scalars(), whole(), whole()],
        out_specs=[whole()] * 2,
        cost_estimate=cost(2**25, 2 * picks * groups * rows * slots),
        compiler_params=grant(6, groups),
        name="plan",
    )(place, routes, route_weights)


def gather_kernel(chosen_ref, weights_ref, *refs, groups):
    table_refs, out_refs = refs[:groups], refs[groups:]
    picks = chosen_ref.shape[0] // groups
    width = out_refs[0].shape[1]
    total = None
    for pick in range(picks):
        picked = None
        for group in range(groups):
            part = jnp.dot(
                chosen_ref[pick * groups + group],
                table_refs[group][...],
                preferred_element_type=F32,
            )
            picked = part if picked is None else picked + part
        picked = picked * weights_ref[:, pick : pick + 1]
        total = picked if total is None else total + picked
    for level, ref in enumerate(out_refs):
        ref[...] = total[:, level * width : (level + 1) * width].astype(BF16)


def gather(chosen, scale, tables, levels):
    groups = len(tables)
    rows, picks = scale.shape[0], chosen.shape[0] // groups
    slots, width = tables[0].shape
    return pl.pallas_call(
        functools.partial(gather_kernel, groups=groups),
        out_shape=[shape_of(rows, width // levels)] * levels,
        in_specs=[whole()] * (2 + groups),
        out_specs=[whole()] * levels,
        cost_estimate=cost(
            2 * picks * groups * slots * rows * width,
            2 * groups * slots * (width + picks * rows) + 2 * rows * width,
        ),
        compiler_params=grant(8),
        name="gather",
    )(chosen, scale, *tables)


def final_kernel(*refs):
    total = refs[0][...].astype(F32)
    for ref in refs[1:-1]:
        total += ref[...].astype(F32)
    refs[-1][...] = total.astype(BF16)


def final(parts):
    rows, width = parts[0].shape
    return pl.pallas_call(
        final_kernel,
        out_shape=shape_of(rows, width),
        in_specs=[whole()] * len(parts),
        out_specs=whole(),
        cost_estimate=cost(2**20, 2 * len(parts) * rows * width),
        compiler_params=grant(4),
        name="final",
    )(*parts)


def shards(
    queries, keys, values, mix_weight, sub_gain, tokens, routes, route_weights,
    expert_gain, gate_weight, up_weight, down_weight,
):
    rows2, width = tokens.shape
    picks = routes.shape[1]
    groups, levels = lax.axis_size("ep"), lax.axis_size("tp") // CORES
    pieces = gate_weight.shape[0]
    experts = groups * pieces
    capacity = 3 * rows2 * picks // (2 * experts)
    half = levels // 2
    tp_index = lax.axis_index("tp")
    spot = jnp.stack([lax.axis_index("ep"), tp_index // CORES, tp_index % CORES])
    place = spot = spot.astype(jnp.int32)

    by_level = [tokens]
    for mask in range(1, levels):
        by_level.append(levels_flip(tokens, mask))
    by_level[0], picked, picked_weights = fetch(tokens, routes.T, route_weights.T, mebibytes=2)
    chosen, scale = plan(
        place, picked, picked_weights, capacity, pieces, experts, groups
    )
    queries, keys, values, scale = lax.optimization_barrier((queries, keys, values, scale))
    bundles = pack(place, queries, keys, values, groups)
    own, other = [], []
    for chunk in range(2):
        some = by_level[chunk * half : (chunk + 1) * half]
        tables = dispatch(place, picked, some, capacity, pieces, experts, groups)
        own.append(exchange(tables))
    bundles = exchange(bundles)
    for chunk in range(2):
        swapped = []
        for table in own[chunk]:
            swapped.append(cores_flip(table))
        other.append(swapped)
    gate_near, up_near = fetch(gate_weight, up_weight, mebibytes=FETCH_GRANT)
    hidden = hidden_units(
        spot, own, other, expert_gain, gate_near, up_near, groups, capacity, width
    )
    halves = []
    for first in (0, half):
        sent, kept = down(
            spot, hidden, down_weight, groups, capacity, width, first, half
        )
        halves.append((kept, cores_flip(sent)))
    values = list(part_levels(*halves[0], half))
    for level in range(1, half):
        values[level] = levels_flip(values[level], level)
    tables = add_cores(*halves[1], groups)
    tables = exchange(tables)
    combined = gather(chosen, scale, tables, half)
    results = []
    for inner, value in enumerate(combined):
        results.append(levels_flip(value, half + inner))
    tables = sum_levels(values, groups)
    tables = exchange(tables)
    results += gather(chosen, scale, tables, 1)
    attended = attention(place, bundles, mix_weight, sub_gain, queries.shape[0])
    attended = exchange(attended)
    moe_out = final(results)
    attn_out = unpack(place, attended, queries.shape[1])
    return (attn_out, moe_out)


def solution(mesh):
    return jax.shard_map(
        shards,
        mesh=mesh,
        in_specs=(
            P("ep", "tp", None),
            P("ep", "tp", None),
            P("ep", "tp", None),
            P("tp"),
            P(),
            P("ep", "tp"),
            P("ep", None),
            P("ep", None),
            P(),
            P("ep", None, "tp"),
            P("ep", None, "tp"),
            P("ep", "tp", None),
        ),
        out_specs=(P("ep", "tp", None), P("ep", "tp")),
        check_vma=False,
    )
```

```python
import functools

import jax
import jax.numpy as jnp
from jax import lax
from jax.experimental import pallas as pl
from jax.experimental.pallas import tpu as pltpu
from jax.sharding import PartitionSpec as P


NEG_FILL = -1e30
SUB_EPS = 1e-05
NORM_EPS = 1e-06
CLAMP_LIMIT = 7.0
GLU_ALPHA = 1.702
OUT_SCALE = 0.8
LOG2E = 1.4426950408889634
CORES = 2
FETCH_GRANT = 44
SPLITS = 2
BF16 = jnp.bfloat16
F32 = jnp.float32


def whole():
    return pl.BlockSpec(memory_space=pltpu.VMEM)


def far():
    return pl.BlockSpec(memory_space=pl.ANY)


def scalars():
    return pl.BlockSpec(memory_space=pltpu.SMEM)


def shape_of(*sizes, dtype=BF16):
    return jax.ShapeDtypeStruct(sizes, dtype)


def grant(mebibytes, groups=4):
    size = min(60, mebibytes * max(1, groups // 4))
    return pltpu.CompilerParams(vmem_limit_bytes=size * 1024 * 1024)


def cost(flops, data, transcendentals=0):
    return pl.CostEstimate(
        flops=int(flops), bytes_accessed=int(data), transcendentals=int(transcendentals)
    )


def flip(value, axis, mask):
    pairs = [(source, source ^ mask) for source in range(lax.axis_size(axis))]
    return lax.ppermute(value, axis, pairs)


def levels_flip(value, mask):
    return flip(value, "tp", CORES * mask)


def cores_flip(value):
    return flip(value, "tp", 1)


def exchange(values):
    out = [values[0]]
    for mask in range(1, len(values)):
        out.append(flip(values[mask], "ep", mask))
    return out


def share_at(part, block, splits):
    return jnp.where(block % 2 == 0, part, splits - 1 - part)


def pack_kernel(place_ref, queries_ref, keys_ref, values_ref, *out_refs):
    place = place_ref[0]
    heads, rows, _ = keys_ref.shape
    splits = len(out_refs) // heads
    share = rows // splits
    for mask, out_ref in enumerate(out_refs):
        target = jnp.bitwise_xor(place, mask)
        head = lax.div(target, splits)
        start = share_at(lax.rem(target, splits), place, splits) * share
        out_ref[:rows] = keys_ref[head]
        out_ref[rows : 2 * rows] = values_ref[head]
        out_ref[2 * rows :] = queries_ref[head, pl.ds(pl.multiple_of(start, share), share)]


def pack(place, queries, keys, values, groups):
    rows, heads, width = queries.shape
    tall = 2 * rows + rows * heads // groups
    return pl.pallas_call(
        pack_kernel,
        out_shape=[shape_of(tall, width)] * groups,
        in_specs=[scalars(), whole(), whole(), whole()],
        out_specs=[whole()] * groups,
        cost_estimate=cost(2**21, 2 * groups * tall * width),
        compiler_params=grant(8),
        name="pack",
    )(place, *[jnp.transpose(value, (1, 0, 2)) for value in (queries, keys, values)])


def attention_kernel(place_ref, mix_ref, *refs, groups, rows, heads, scale):
    bundle_refs, gain_ref = refs[:groups], refs[groups]
    out_refs = refs[groups + 1 : 2 * groups + 1]
    bundle, outputs, scores, arrivals = refs[2 * groups + 1 :]
    place = place_ref[0]
    copies = []
    for mask in range(groups):
        copies.append(
            pltpu.make_async_copy(
                bundle_refs[mask], bundle.at[jnp.bitwise_xor(place, mask)], arrivals.at[mask]
            )
        )
    for copy in copies:
        copy.start()
    share, width = out_refs[0].shape
    splits = groups // heads
    mix = mix_ref[lax.div(place, splits)]
    part = lax.rem(place, splits)
    half = width // 2
    lane = lax.broadcasted_iota(jnp.int32, (share, width), 1)
    row = lax.broadcasted_iota(jnp.int32, (share, rows), 0)
    column = lax.broadcasted_iota(jnp.int32, (share, rows), 1)
    contract = (((1,), (1,)), ((), ()))
    factor = scale * LOG2E
    for copy in copies:
        copy.wait()
    tops = [None, None]
    for block in range(groups):
        visible = column <= row + (part if block % 2 == 0 else splits - 1 - part) * share
        queries = bundle[block, 2 * rows :, :]
        empty = jnp.zeros_like(queries)
        for side in range(2):
            query = jnp.where((lane < half) if side == 0 else (lane >= half), queries, empty)
            top = jnp.full((share, width), NEG_FILL, F32)
            for other in range(block + 1):
                score = lax.dot_general(
                    query, bundle[other, :rows, :], contract, preferred_element_type=F32
                )
                if other == block:
                    score = jnp.where(visible, score, NEG_FILL)
                scores[side, :, other * rows : (other + 1) * rows] = score
                for start in range(0, rows, width):
                    top = jnp.maximum(top, score[:, start : start + width])
            tops[side] = jnp.max(top, axis=-1, keepdims=True)
        sums = []
        for side in range(2):
            top = tops[side]
            total = jnp.zeros((share, width), F32)
            weighted = jnp.zeros((share, width), F32)
            for other in range(block + 1):
                score = scores[side, :, other * rows : (other + 1) * rows]
                weight = jnp.exp2((score - top) * factor)
                for start in range(0, rows, width):
                    total += weight[:, start : start + width]
                weighted += jnp.dot(
                    weight.astype(BF16),
                    bundle[other, rows : 2 * rows, :],
                    preferred_element_type=F32,
                )
            sums.append(weighted / jnp.sum(total, axis=-1, keepdims=True))
        blend = sums[0] - mix * sums[1]
        mean = jnp.mean(blend * blend, axis=-1, keepdims=True)
        scaled = blend * lax.rsqrt(mean + SUB_EPS)
        outputs[block] = (scaled * gain_ref[...] * OUT_SCALE).astype(BF16)
    for mask in range(groups):
        out_refs[mask][...] = outputs[jnp.bitwise_xor(place, mask)]


def attention(place, bundles, mix_weight, sub_gain, rows):
    groups, heads = len(bundles), mix_weight.shape[0]
    tall, width = bundles[0].shape
    share = tall - 2 * rows
    pairs = groups * (groups + 1) // 2 * share * rows * 2
    return pl.pallas_call(
        functools.partial(
            attention_kernel, groups=groups, rows=rows, heads=heads, scale=(width // 2) ** -0.5
        ),
        out_shape=[shape_of(share, width)] * groups,
        in_specs=[scalars(), scalars()] + [far()] * groups + [whole()],
        out_specs=[whole()] * groups,
        scratch_shapes=[
            pltpu.VMEM((groups, tall, width), BF16),
            pltpu.VMEM((groups, share, width), BF16),
            pltpu.VMEM((2, share, groups * rows), F32),
            pltpu.SemaphoreType.DMA((groups,)),
        ],
        cost_estimate=cost(pairs * 4 * width, 2 * groups * tall * width, pairs),
        compiler_params=grant(16, groups),
        name="attention",
    )(place, mix_weight, *bundles, sub_gain[None, :])


def unpack_kernel(place_ref, *refs):
    part_refs, out_ref = refs[:-1], refs[-1]
    place = place_ref[0]
    groups, share = len(part_refs), part_refs[0].shape[0]
    splits = groups // out_ref.shape[0]
    for mask, ref in enumerate(part_refs):
        source = jnp.bitwise_xor(place, mask)
        start = share_at(lax.rem(source, splits), place, splits) * share
        out_ref[lax.div(source, splits), pl.ds(pl.multiple_of(start, share), share)] = ref[...]


def unpack(place, parts, heads):
    groups = len(parts)
    share, width = parts[0].shape
    rows = share * groups // heads
    by_head = pl.pallas_call(
        unpack_kernel,
        out_shape=shape_of(heads, rows, width),
        in_specs=[scalars()] + [whole()] * groups,
        out_specs=whole(),
        cost_estimate=cost(2**20, 4 * heads * rows * width),
        compiler_params=grant(4),
        name="unpack",
    )(place, *parts)
    return jnp.transpose(by_head, (1, 0, 2))


def ranks(named, strictly, axis):
    table = named.astype(F32).astype(BF16)
    earlier = strictly.astype(F32).astype(BF16)
    pair = (table, earlier) if axis == 1 else (earlier, table)
    return jnp.dot(*pair, preferred_element_type=F32)


def dispatch_kernel(place_ref, routes_ref, *refs, capacity, pieces, experts, groups):
    level_refs, out_refs = refs[:-groups], refs[-groups:]
    place = place_ref[0]
    rows, width = level_refs[0].shape
    picks = routes_ref.shape[0]
    tall = max(experts, 16)
    expert = lax.broadcasted_iota(jnp.int32, (tall, rows), 0)
    named = jnp.zeros((tall, rows), jnp.bool_)
    for pick in range(picks):
        named = named | (routes_ref[pick : pick + 1, :] == expert)
    first = lax.broadcasted_iota(jnp.int32, (rows, rows), 0)
    second = lax.broadcasted_iota(jnp.int32, (rows, rows), 1)
    rank = ranks(named, first < second, 1)
    targets = []
    for pick in range(picks):
        route = routes_ref[pick : pick + 1, :]
        mine = jnp.sum(jnp.where(expert == route, rank, 0.0), axis=0, keepdims=True)
        targets.append(route * capacity + mine.astype(jnp.int32))
    slots = pieces * capacity
    slot = lax.broadcasted_iota(jnp.int32, (slots, rows), 0)
    for mask in range(groups):
        here = slot + jnp.bitwise_xor(place, mask) * slots
        chosen = jnp.zeros((slots, rows), jnp.bool_)
        for pick in range(picks):
            chosen = chosen | (here == targets[pick])
        onehot = chosen.astype(F32).astype(BF16)
        for level, ref in enumerate(level_refs):
            out_refs[mask][:, level * width : (level + 1) * width] = jnp.dot(
                onehot, ref[...], preferred_element_type=F32
            ).astype(BF16)


def dispatch(place, routes, by_level, capacity, pieces, experts, groups):
    rows, width = by_level[0].shape
    slots, wide = pieces * capacity, len(by_level) * width
    return pl.pallas_call(
        functools.partial(
            dispatch_kernel, capacity=capacity, pieces=pieces, experts=experts, groups=groups
        ),
        out_shape=[shape_of(slots, wide)] * groups,
        in_specs=[scalars(), whole()] + [whole()] * len(by_level),
        out_specs=[whole()] * groups,
        cost_estimate=cost(2 * groups * slots * rows * wide, 4 * groups * slots * wide),
        compiler_params=grant(8),
        name="dispatch",
    )(place, routes, *by_level)


def block_start(spot_ref, level, side, width):
    core = spot_ref[2] if side == 0 else 1 - spot_ref[2]
    return (CORES * jnp.bitwise_xor(spot_ref[1], level) + core) * width


def fetch_kernel(*refs):
    count = (len(refs) - 1) // 2
    arrivals = refs[-1]
    copies = []
    for source, target in zip(refs[:count], refs[count : 2 * count]):
        count = 1 if len(source.shape) < 3 else SPLITS
        rows = source.shape[-2] // count
        for index in range(source.shape[0] * count if count > 1 else 1):
            part = (
                (index // count, pl.ds(index % count * rows, rows)) if count > 1 else ()
            )
            copies.append(
                pltpu.make_async_copy(source.at[part], target.at[part], arrivals.at[len(copies)])
            )
    for copy in copies:
        copy.start()
    for copy in copies:
        copy.wait()


def fetch(*arrays, mebibytes):
    return pl.pallas_call(
        fetch_kernel,
        out_shape=[shape_of(*array.shape, dtype=array.dtype) for array in arrays],
        in_specs=[far()] * len(arrays),
        out_specs=[whole()] * len(arrays),
        scratch_shapes=[pltpu.SemaphoreType.DMA((2 * SPLITS * len(arrays),))],
        cost_estimate=cost(2**20, sum(4 * array.size for array in arrays)),
        compiler_params=grant(mebibytes),
    )(*arrays)


def hidden_kernel(spot_ref, *refs, groups, capacity, width, chunk, last):
    count = CORES * groups
    slot_refs = refs[:count]
    gain_ref, gate_ref, up_ref = refs[count : count + 3]
    rest = refs[count + 3 :]
    pieces, total_width, ff = gate_ref.shape
    tile = 256 if ff % 256 == 0 else ff
    span = slot_refs[0].shape[1] // width
    depth = CORES * span * width
    first = lax.div(spot_ref[1], span)
    base = pl.multiple_of((first if chunk == 0 else jnp.bitwise_xor(first, chunk)) * depth, depth)
    if last:
        sums_ref, squares_ref, hidden_ref, normed = rest
    else:
        sums_ref, squares_ref, normed = rest
    factors = [[None] * groups for _ in range(pieces)]
    slots = pieces * capacity
    for group in range(groups):
        squares = jnp.zeros((slots, 1), F32)
        for side in range(CORES):
            ref = slot_refs[side * groups + group]
            for inner in range(span):
                floats = ref[:, inner * width : (inner + 1) * width].astype(F32)
                squares += jnp.sum(floats * floats, axis=-1, keepdims=True)
                start = block_start(spot_ref, chunk * span + inner, side, width)
                gain = gain_ref[:, pl.ds(pl.multiple_of(start, width), width)]
                value = (floats * gain).astype(BF16)
                place = pl.ds(pl.multiple_of(start - base, width), width)
                for piece in range(pieces):
                    normed[piece, group * capacity : (group + 1) * capacity, place] = value[
                        piece * capacity : (piece + 1) * capacity
                    ]
        rows = slice(group * slots, (group + 1) * slots)
        if last:
            squares += squares_ref[rows, 0:1]
            factor = lax.rsqrt(squares / total_width + NORM_EPS)
            for piece in range(pieces):
                factors[piece][group] = factor[piece * capacity : (piece + 1) * capacity]
        else:
            squares_ref[rows] = jnp.broadcast_to(squares, (slots, squares_ref.shape[1]))
    for piece in range(pieces):
        factor = jnp.concatenate(factors[piece], axis=0) if last else None
        for start in range(0, ff, tile):
            columns = slice(start, start + tile)
            pair = []
            for kind, ref in enumerate((gate_ref, up_ref)):
                value = jnp.dot(
                    normed[piece],
                    ref[piece, pl.ds(base, depth), columns],
                    preferred_element_type=F32,
                )
                if last:
                    pair.append((value + sums_ref[kind, piece, :, columns]) * factor)
                else:
                    sums_ref[kind, piece, :, columns] = value
            if last:
                gate = jnp.minimum(pair[0], CLAMP_LIMIT)
                up = jnp.clip(pair[1], -CLAMP_LIMIT, CLAMP_LIMIT)
                hidden_ref[piece, :, columns] = (
                    (up + 1.0) * gate * jax.nn.sigmoid(GLU_ALPHA * gate)
                ).astype(BF16)


def hidden_units(spot, tables, prior, gain, gate, up, groups, capacity, width, chunk):
    pieces, _, ff = gate.shape
    rows, depth = groups * capacity, CORES * tables[0].shape[1]
    last = prior is not None
    sums = [shape_of(2, pieces, rows, ff, dtype=F32), shape_of(pieces * rows, 128, dtype=F32)]
    inputs = list(tables) + [gain[None, :], gate, up] + (list(prior) if last else [])
    return pl.pallas_call(
        functools.partial(
            hidden_kernel, groups=groups, capacity=capacity, width=width, chunk=chunk, last=last
        ),
        out_shape=shape_of(pieces, rows, ff) if last else sums,
        in_specs=[scalars()] + [whole()] * len(inputs),
        out_specs=whole() if last else [whole()] * 2,
        scratch_shapes=[pltpu.VMEM((pieces, rows, depth), BF16)],
        cost_estimate=cost(
            4 * pieces * rows * depth * ff, 4 * pieces * depth * (ff + rows), pieces * rows * ff
        ),
        compiler_params=grant(14),
    )(spot, *inputs)


def down_kernel(
    spot_ref, hidden_ref, down_ref, sent_ref, kept_ref, *, groups, capacity, width, first
):
    pieces = hidden_ref.shape[0]
    for side, ref in ((1, sent_ref), (0, kept_ref)):
        for piece in range(pieces):
            for inner in range(ref.shape[1] // width):
                start = block_start(spot_ref, first + inner, side, width)
                value = jnp.dot(
                    hidden_ref[piece],
                    down_ref[piece, :, pl.ds(pl.multiple_of(start, width), width)],
                    preferred_element_type=F32,
                ).astype(BF16)
                for group in range(groups):
                    row = (group * pieces + piece) * capacity
                    ref[row : row + capacity, inner * width : (inner + 1) * width] = value[
                        group * capacity : (group + 1) * capacity
                    ]


def down(spot, hidden, down_weight, groups, capacity, width, first, span):
    pieces, rows, ff = hidden.shape
    part = span * width
    return pl.pallas_call(
        functools.partial(down_kernel, groups=groups, capacity=capacity, width=width, first=first),
        out_shape=[shape_of(pieces * rows, part)] * 2,
        in_specs=[scalars(), whole(), whole()],
        out_specs=[whole()] * 2,
        cost_estimate=cost(
            2 * CORES * pieces * rows * ff * part, 2 * CORES * pieces * part * (ff + rows)
        ),
        compiler_params=grant(12),
        name="down",
    )(spot, hidden, down_weight)


def add_kernel(kept_ref, partner_ref, *out_refs):
    rows = out_refs[0].shape[0]
    for group, ref in enumerate(out_refs):
        place = slice(group * rows, (group + 1) * rows)
        ref[...] = (kept_ref[place].astype(F32) + partner_ref[place].astype(F32)).astype(BF16)


def add_cores(kept, partner, groups):
    rows, width = kept.shape
    return pl.pallas_call(
        add_kernel,
        out_shape=[shape_of(rows // groups, width)] * groups,
        in_specs=[whole()] * 2,
        out_specs=[whole()] * groups,
        cost_estimate=cost(2**21, 6 * rows * width),
        compiler_params=grant(6),
        name="add_cores",
    )(kept, partner)


def part_kernel(kept_ref, partner_ref, mine_ref, *out_refs):
    width = mine_ref.shape[1]
    for level, ref in enumerate((mine_ref,) + out_refs):
        place = slice(level * width, (level + 1) * width)
        total = kept_ref[:, place].astype(F32) + partner_ref[:, place].astype(F32)
        ref[...] = total.astype(ref.dtype)


def part_levels(kept, partner, levels):
    rows, width = kept.shape
    own = width // levels
    return pl.pallas_call(
        part_kernel,
        out_shape=[shape_of(rows, own, dtype=F32)] + [shape_of(rows, own)] * (levels - 1),
        in_specs=[whole()] * 2,
        out_specs=[whole()] * levels,
        cost_estimate=cost(2**21, 6 * rows * width),
        compiler_params=grant(6),
        name="part_levels",
    )(kept, partner)


def sum_kernel(*refs, groups):
    value_refs, out_refs = refs[:-groups], refs[-groups:]
    rows = out_refs[0].shape[0]
    for group, ref in enumerate(out_refs):
        place = slice(group * rows, (group + 1) * rows)
        total = value_refs[0][place]
        for value_ref in value_refs[1:]:
            total += value_ref[place].astype(F32)
        ref[...] = total.astype(BF16)


def sum_levels(values, groups):
    rows, width = values[0].shape
    return pl.pallas_call(
        functools.partial(sum_kernel, groups=groups),
        out_shape=[shape_of(rows // groups, width)] * groups,
        in_specs=[whole()] * len(values),
        out_specs=[whole()] * groups,
        cost_estimate=cost(2**21, 6 * rows * width),
        compiler_params=grant(6),
        name="sum_levels",
    )(*values)


def plan_kernel(
    place_ref, routes_ref, weights_ref, out_ref, scale_ref, *, capacity, pieces, experts
):
    picks, rows = routes_ref.shape
    slots = out_ref.shape[2]
    groups = out_ref.shape[0] // picks
    wide = max(experts, 128)
    first = lax.broadcasted_iota(jnp.int32, (rows, rows), 0)
    second = lax.broadcasted_iota(jnp.int32, (rows, rows), 1)

    def column(row):
        return jnp.sum(jnp.where(first == second, row, 0.0), axis=1, keepdims=True)

    expert = lax.broadcasted_iota(jnp.int32, (rows, wide), 1)
    named = jnp.zeros((rows, wide), jnp.bool_)
    scale = jnp.zeros((rows, scale_ref.shape[1]), F32)
    lane = lax.broadcasted_iota(jnp.int32, scale.shape, 1)
    routes = []
    for pick in range(picks):
        routes.append(column(routes_ref[pick : pick + 1, :].astype(F32)).astype(jnp.int32))
        named = named | (routes[pick] == expert)
        scale = jnp.where(lane == pick, column(weights_ref[pick : pick + 1, :]), scale)
    scale_ref[...] = scale
    rank = ranks(named, second < first, 0)
    slot = lax.broadcasted_iota(jnp.int32, (rows, slots), 1)
    for pick in range(picks):
        mine = jnp.sum(jnp.where(expert == routes[pick], rank, 0.0), axis=1, keepdims=True)
        target = routes[pick] * capacity + mine.astype(jnp.int32)
        for mask in range(groups):
            here = slot + jnp.bitwise_xor(place_ref[0], mask) * slots
            out_ref[pick * groups + mask] = (here == target).astype(F32).astype(BF16)


def plan(place, routes, route_weights, capacity, pieces, experts, groups):
    picks, rows = routes.shape
    slots = pieces * capacity
    return pl.pallas_call(
        functools.partial(plan_kernel, capacity=capacity, pieces=pieces, experts=experts),
        out_shape=[shape_of(picks * groups, rows, slots), shape_of(rows, 128, dtype=F32)],
        in_specs=[scalars(), whole(), whole()],
        out_specs=[whole()] * 2,
        cost_estimate=cost(2**25, 2 * picks * groups * rows * slots),
        compiler_params=grant(6, groups),
        name="plan",
    )(place, routes, route_weights)


def gather_rows(chosen_ref, scale_ref, table_refs):
    groups = len(table_refs)
    total = None
    for pick in range(chosen_ref.shape[0] // groups):
        picked = None
        for group in range(groups):
            part = jnp.dot(
                chosen_ref[pick * groups + group],
                table_refs[group][...],
                preferred_element_type=F32,
            )
            picked = part if picked is None else picked + part
        picked = picked * scale_ref[:, pick : pick + 1]
        total = picked if total is None else total + picked
    return total


def gather_kernel(chosen_ref, scale_ref, *refs, groups):
    total = gather_rows(chosen_ref, scale_ref, refs[:groups])
    out_refs = refs[groups:]
    width = out_refs[0].shape[1]
    for level, ref in enumerate(out_refs):
        ref[...] = total[:, level * width : (level + 1) * width].astype(BF16)


def gather(chosen, scale, tables, levels):
    groups = len(tables)
    rows, picks = scale.shape[0], chosen.shape[0] // groups
    slots, width = tables[0].shape
    return pl.pallas_call(
        functools.partial(gather_kernel, groups=groups),
        out_shape=[shape_of(rows, width // levels)] * levels,
        in_specs=[whole()] * (2 + groups),
        out_specs=[whole()] * levels,
        cost_estimate=cost(
            2 * picks * groups * slots * rows * width,
            2 * groups * slots * (width + picks * rows) + 2 * rows * width,
        ),
        compiler_params=grant(8),
        name="gather",
    )(chosen, scale, *tables)


def final_kernel(chosen_ref, scale_ref, *refs, groups):
    total = gather_rows(chosen_ref, scale_ref, refs[:groups])
    for ref in refs[groups:-1]:
        total += ref[...].astype(F32)
    refs[-1][...] = total.astype(BF16)


def final(chosen, scale, tables, parts):
    rows, width = parts[0].shape
    groups = len(tables)
    return pl.pallas_call(
        functools.partial(final_kernel, groups=groups),
        out_shape=shape_of(rows, width),
        in_specs=[whole()] * (2 + groups + len(parts)),
        out_specs=whole(),
        cost_estimate=cost(2**28, 2 * (groups + len(parts)) * rows * width),
        compiler_params=grant(8),
        name="final",
    )(chosen, scale, *tables, *parts)


def shards(
    queries, keys, values, mix_weight, sub_gain, tokens, routes, route_weights,
    expert_gain, gate_weight, up_weight, down_weight,
):
    rows2, width = tokens.shape
    picks = routes.shape[1]
    groups, levels = lax.axis_size("ep"), lax.axis_size("tp") // CORES
    pieces = gate_weight.shape[0]
    experts = groups * pieces
    capacity = 3 * rows2 * picks // (2 * experts)
    half = levels // 2
    tp_index = lax.axis_index("tp")
    spot = jnp.stack([lax.axis_index("ep"), tp_index // CORES, tp_index % CORES])
    place = spot = spot.astype(jnp.int32)

    by_level = [tokens]
    for mask in range(1, levels):
        by_level.append(levels_flip(tokens, mask))
    (gate_near,) = fetch(gate_weight, mebibytes=FETCH_GRANT)
    by_level[0], picked, picked_weights = fetch(tokens, routes.T, route_weights.T, mebibytes=2)
    chosen, scale = plan(
        place, picked, picked_weights, capacity, pieces, experts, groups
    )
    queries, keys, values, scale = lax.optimization_barrier((queries, keys, values, scale))
    bundles = pack(place, queries, keys, values, groups)
    own, other = [], []
    for chunk in range(2):
        some = by_level[chunk * half : (chunk + 1) * half]
        tables = dispatch(place, picked, some, capacity, pieces, experts, groups)
        own.append(exchange(tables))
    bundles = exchange(bundles)
    for chunk in range(2):
        swapped = []
        for table in own[chunk]:
            swapped.append(cores_flip(table))
        other.append(swapped)
    (up_near,) = fetch(up_weight, mebibytes=FETCH_GRANT)
    hidden = None
    for chunk in range(2):
        hidden = hidden_units(
            spot, own[chunk] + other[chunk], hidden, expert_gain, gate_near, up_near,
            groups, capacity, width, chunk,
        )
    halves = []
    for first in (0, half):
        sent, kept = down(
            spot, hidden, down_weight, groups, capacity, width, first, half
        )
        halves.append((kept, cores_flip(sent)))
    values = list(part_levels(*halves[0], half))
    for level in range(1, half):
        values[level] = levels_flip(values[level], level)
    tables = add_cores(*halves[1], groups)
    tables = exchange(tables)
    combined = gather(chosen, scale, tables, half)
    results = []
    for inner, value in enumerate(combined):
        results.append(levels_flip(value, half + inner))
    tables = sum_levels(values, groups)
    tables = exchange(tables)
    attended = attention(place, bundles, mix_weight, sub_gain, queries.shape[0])
    attended = exchange(attended)
    moe_out = final(chosen, scale, tables, results)
    attn_out = unpack(place, attended, queries.shape[1])
    return (attn_out, moe_out)


def solution(mesh):
    return jax.shard_map(
        shards,
        mesh=mesh,
        in_specs=(
            P("ep", "tp", None),
            P("ep", "tp", None),
            P("ep", "tp", None),
            P("tp"),
            P(),
            P("ep", "tp"),
            P("ep", None),
            P("ep", None),
            P(),
            P("ep", None, "tp"),
            P("ep", None, "tp"),
            P("ep", "tp", None),
        ),
        out_specs=(P("ep", "tp", None), P("ep", "tp")),
        check_vma=False,
    )
```

```python
import functools

import jax
import jax.numpy as jnp
from jax import lax
from jax.experimental import pallas as pl
from jax.experimental.pallas import tpu as pltpu
from jax.sharding import PartitionSpec as P


NEG_FILL = -1e30
SUB_EPS = 1e-05
NORM_EPS = 1e-06
CLAMP_LIMIT = 7.0
GLU_ALPHA = 1.702
OUT_SCALE = 0.8
LOG2E = 1.4426950408889634
CORES = 2
GATE_GRANT = 46
UP_GRANT = 44
SPLITS = 2
BF16 = jnp.bfloat16
F32 = jnp.float32


def whole():
    return pl.BlockSpec(memory_space=pltpu.VMEM)


def far():
    return pl.BlockSpec(memory_space=pl.ANY)


def scalars():
    return pl.BlockSpec(memory_space=pltpu.SMEM)


def shape_of(*sizes, dtype=BF16):
    return jax.ShapeDtypeStruct(sizes, dtype)


def grant(mebibytes, groups=4):
    size = min(60, mebibytes * max(1, groups // 4))
    return pltpu.CompilerParams(vmem_limit_bytes=size * 1024 * 1024)


def cost(flops, data, transcendentals=0):
    return pl.CostEstimate(
        flops=int(flops), bytes_accessed=int(data), transcendentals=int(transcendentals)
    )


def flip(value, axis, mask):
    pairs = [(source, source ^ mask) for source in range(lax.axis_size(axis))]
    return lax.ppermute(value, axis, pairs)


def levels_flip(value, mask):
    return flip(value, "tp", CORES * mask)


def cores_flip(value):
    return flip(value, "tp", 1)


def exchange(values):
    out = [values[0]]
    for mask in range(1, len(values)):
        out.append(flip(values[mask], "ep", mask))
    return out


def share_at(part, block, splits):
    return jnp.where(block % 2 == 0, part, splits - 1 - part)


def pack_kernel(place_ref, queries_ref, keys_ref, values_ref, *out_refs):
    place = place_ref[0]
    heads, rows, _ = keys_ref.shape
    splits = len(out_refs) // heads
    share = rows // splits
    for mask, out_ref in enumerate(out_refs):
        target = jnp.bitwise_xor(place, mask)
        head = lax.div(target, splits)
        start = share_at(lax.rem(target, splits), place, splits) * share
        out_ref[:rows] = keys_ref[head]
        out_ref[rows : 2 * rows] = values_ref[head]
        out_ref[2 * rows :] = queries_ref[head, pl.ds(pl.multiple_of(start, share), share)]


def pack(place, queries, keys, values, groups):
    rows, heads, width = queries.shape
    tall = 2 * rows + rows * heads // groups
    return pl.pallas_call(
        pack_kernel,
        out_shape=[shape_of(tall, width)] * groups,
        in_specs=[scalars(), whole(), whole(), whole()],
        out_specs=[whole()] * groups,
        cost_estimate=cost(2**21, 2 * groups * tall * width),
        compiler_params=grant(8),
        name="pack",
    )(place, *[jnp.transpose(value, (1, 0, 2)) for value in (queries, keys, values)])


def attention_kernel(place_ref, mix_ref, *refs, groups, rows, heads, scale):
    bundle_refs, gain_ref = refs[:groups], refs[groups]
    out_refs = refs[groups + 1 : 2 * groups + 1]
    bundle, outputs, scores, turned, arrivals = refs[2 * groups + 1 :]
    place = place_ref[0]
    copies = []
    for mask in range(groups):
        copies.append(
            pltpu.make_async_copy(
                bundle_refs[mask], bundle.at[jnp.bitwise_xor(place, mask)], arrivals.at[mask]
            )
        )
    for copy in copies:
        copy.start()
    share, width = out_refs[0].shape
    splits = groups // heads
    mix = mix_ref[lax.div(place, splits)]
    part = lax.rem(place, splits)
    half = width // 2
    lane = lax.broadcasted_iota(jnp.int32, (share, width), 1)
    row = lax.broadcasted_iota(jnp.int32, (share, rows), 0)
    column = lax.broadcasted_iota(jnp.int32, (share, rows), 1)
    factor = scale * LOG2E
    for copy in copies:
        copy.wait()
    for block in range(groups):
        turned[block] = bundle[block, :rows, :].T
    tops = [None, None]
    for block in range(groups):
        visible = column <= row + (part if block % 2 == 0 else splits - 1 - part) * share
        queries = bundle[block, 2 * rows :, :]
        empty = jnp.zeros_like(queries)
        for side in range(2):
            query = jnp.where((lane < half) if side == 0 else (lane >= half), queries, empty)
            top = jnp.full((share, width), NEG_FILL, F32)
            for other in range(block + 1):
                score = jnp.dot(query, turned[other], preferred_element_type=F32)
                if other == block:
                    score = jnp.where(visible, score, NEG_FILL)
                scores[side, :, other * rows : (other + 1) * rows] = score
                for start in range(0, rows, width):
                    top = jnp.maximum(top, score[:, start : start + width])
            tops[side] = jnp.max(top, axis=-1, keepdims=True)
        sums = []
        for side in range(2):
            top = tops[side]
            total = jnp.zeros((share, width), F32)
            weighted = jnp.zeros((share, width), F32)
            for other in range(block + 1):
                score = scores[side, :, other * rows : (other + 1) * rows]
                weight = jnp.exp2((score - top) * factor)
                for start in range(0, rows, width):
                    total += weight[:, start : start + width]
                weighted += jnp.dot(
                    weight.astype(BF16),
                    bundle[other, rows : 2 * rows, :],
                    preferred_element_type=F32,
                )
            sums.append(weighted / jnp.sum(total, axis=-1, keepdims=True))
        blend = sums[0] - mix * sums[1]
        mean = jnp.mean(blend * blend, axis=-1, keepdims=True)
        scaled = blend * lax.rsqrt(mean + SUB_EPS)
        outputs[block] = (scaled * gain_ref[...] * OUT_SCALE).astype(BF16)
    for mask in range(groups):
        out_refs[mask][...] = outputs[jnp.bitwise_xor(place, mask)]


def attention(place, bundles, mix_weight, sub_gain, rows):
    groups, heads = len(bundles), mix_weight.shape[0]
    tall, width = bundles[0].shape
    share = tall - 2 * rows
    pairs = groups * (groups + 1) // 2 * share * rows * 2
    return pl.pallas_call(
        functools.partial(
            attention_kernel, groups=groups, rows=rows, heads=heads, scale=(width // 2) ** -0.5
        ),
        out_shape=[shape_of(share, width)] * groups,
        in_specs=[scalars(), scalars()] + [far()] * groups + [whole()],
        out_specs=[whole()] * groups,
        scratch_shapes=[
            pltpu.VMEM((groups, tall, width), BF16),
            pltpu.VMEM((groups, share, width), BF16),
            pltpu.VMEM((2, share, groups * rows), F32),
            pltpu.VMEM((groups, width, rows), BF16),
            pltpu.SemaphoreType.DMA((groups,)),
        ],
        cost_estimate=cost(pairs * 4 * width, 2 * groups * tall * width, pairs),
        compiler_params=grant(16, groups),
        name="attention",
    )(place, mix_weight, *bundles, sub_gain[None, :])


def unpack_kernel(place_ref, *refs):
    part_refs, out_ref = refs[:-1], refs[-1]
    place = place_ref[0]
    groups, share = len(part_refs), part_refs[0].shape[0]
    splits = groups // out_ref.shape[0]
    for mask, ref in enumerate(part_refs):
        source = jnp.bitwise_xor(place, mask)
        start = share_at(lax.rem(source, splits), place, splits) * share
        out_ref[lax.div(source, splits), pl.ds(pl.multiple_of(start, share), share)] = ref[...]


def unpack(place, parts, heads):
    groups = len(parts)
    share, width = parts[0].shape
    rows = share * groups // heads
    by_head = pl.pallas_call(
        unpack_kernel,
        out_shape=shape_of(heads, rows, width),
        in_specs=[scalars()] + [whole()] * groups,
        out_specs=whole(),
        cost_estimate=cost(2**20, 4 * heads * rows * width),
        compiler_params=grant(4),
        name="unpack",
    )(place, *parts)
    return jnp.transpose(by_head, (1, 0, 2))


def ranks(named, strictly, axis):
    table = named.astype(F32).astype(BF16)
    earlier = strictly.astype(F32).astype(BF16)
    pair = (table, earlier) if axis == 1 else (earlier, table)
    return jnp.dot(*pair, preferred_element_type=F32)


def dispatch_kernel(place_ref, routes_ref, *refs, capacity, pieces, experts, groups):
    level_refs, out_refs = refs[:-groups], refs[-groups:]
    place = place_ref[0]
    rows, width = level_refs[0].shape
    picks = routes_ref.shape[0]
    tall = max(experts, 16)
    expert = lax.broadcasted_iota(jnp.int32, (tall, rows), 0)
    named = jnp.zeros((tall, rows), jnp.bool_)
    for pick in range(picks):
        named = named | (routes_ref[pick : pick + 1, :] == expert)
    first = lax.broadcasted_iota(jnp.int32, (rows, rows), 0)
    second = lax.broadcasted_iota(jnp.int32, (rows, rows), 1)
    rank = ranks(named, first < second, 1)
    targets = []
    for pick in range(picks):
        route = routes_ref[pick : pick + 1, :]
        mine = jnp.sum(jnp.where(expert == route, rank, 0.0), axis=0, keepdims=True)
        targets.append(route * capacity + mine.astype(jnp.int32))
    slots = pieces * capacity
    slot = lax.broadcasted_iota(jnp.int32, (slots, rows), 0)
    for mask in range(groups):
        here = slot + jnp.bitwise_xor(place, mask) * slots
        chosen = jnp.zeros((slots, rows), jnp.bool_)
        for pick in range(picks):
            chosen = chosen | (here == targets[pick])
        onehot = chosen.astype(F32).astype(BF16)
        for level, ref in enumerate(level_refs):
            out_refs[mask][:, level * width : (level + 1) * width] = jnp.dot(
                onehot, ref[...], preferred_element_type=F32
            ).astype(BF16)


def dispatch(place, routes, by_level, capacity, pieces, experts, groups):
    rows, width = by_level[0].shape
    slots, wide = pieces * capacity, len(by_level) * width
    return pl.pallas_call(
        functools.partial(
            dispatch_kernel, capacity=capacity, pieces=pieces, experts=experts, groups=groups
        ),
        out_shape=[shape_of(slots, wide)] * groups,
        in_specs=[scalars(), whole()] + [whole()] * len(by_level),
        out_specs=[whole()] * groups,
        cost_estimate=cost(2 * groups * slots * rows * wide, 4 * groups * slots * wide),
        compiler_params=grant(8),
        name="dispatch",
    )(place, routes, *by_level)


def block_start(spot_ref, level, side, width):
    core = spot_ref[2] if side == 0 else 1 - spot_ref[2]
    return (CORES * jnp.bitwise_xor(spot_ref[1], level) + core) * width


def fetch_kernel(*refs):
    count = (len(refs) - 1) // 2
    arrivals = refs[-1]
    copies = []
    for source, target in zip(refs[:count], refs[count : 2 * count]):
        count = 1 if len(source.shape) < 3 else SPLITS
        rows = source.shape[-2] // count
        for index in range(source.shape[0] * count if count > 1 else 1):
            part = (
                (index // count, pl.ds(index % count * rows, rows)) if count > 1 else ()
            )
            copies.append(
                pltpu.make_async_copy(source.at[part], target.at[part], arrivals.at[len(copies)])
            )
    for copy in copies:
        copy.start()
    for copy in copies:
        copy.wait()


def fetch(*arrays, mebibytes):
    return pl.pallas_call(
        fetch_kernel,
        out_shape=[shape_of(*array.shape, dtype=array.dtype) for array in arrays],
        in_specs=[far()] * len(arrays),
        out_specs=[whole()] * len(arrays),
        scratch_shapes=[pltpu.SemaphoreType.DMA((2 * SPLITS * len(arrays),))],
        cost_estimate=cost(2**20, sum(4 * array.size for array in arrays)),
        compiler_params=grant(mebibytes),
    )(*arrays)


def hidden_kernel(spot_ref, *refs, groups, capacity, width, chunk, last):
    count = CORES * groups
    slot_refs = refs[:count]
    gain_ref, gate_ref, up_ref = refs[count : count + 3]
    rest = refs[count + 3 :]
    pieces, total_width, ff = gate_ref.shape
    tile = 256 if ff % 256 == 0 else ff
    span = slot_refs[0].shape[1] // width
    depth = CORES * span * width
    first = lax.div(spot_ref[1], span)
    base = pl.multiple_of((first if chunk == 0 else jnp.bitwise_xor(first, chunk)) * depth, depth)
    if last:
        sums_ref, squares_ref, down_ref, hidden_ref, sent_ref, kept_ref, normed = rest
    else:
        sums_ref, squares_ref, normed = rest
    factors = [[None] * groups for _ in range(pieces)]
    slots = pieces * capacity
    for group in range(groups):
        squares = jnp.zeros((slots, 1), F32)
        for side in range(CORES):
            ref = slot_refs[side * groups + group]
            for inner in range(span):
                floats = ref[:, inner * width : (inner + 1) * width].astype(F32)
                squares += jnp.sum(floats * floats, axis=-1, keepdims=True)
                start = block_start(spot_ref, chunk * span + inner, side, width)
                gain = gain_ref[:, pl.ds(pl.multiple_of(start, width), width)]
                value = (floats * gain).astype(BF16)
                place = pl.ds(pl.multiple_of(start - base, width), width)
                for piece in range(pieces):
                    normed[piece, group * capacity : (group + 1) * capacity, place] = value[
                        piece * capacity : (piece + 1) * capacity
                    ]
        rows = slice(group * slots, (group + 1) * slots)
        if last:
            squares += squares_ref[rows, 0:1]
            factor = lax.rsqrt(squares / total_width + NORM_EPS)
            for piece in range(pieces):
                factors[piece][group] = factor[piece * capacity : (piece + 1) * capacity]
        else:
            squares_ref[rows] = jnp.broadcast_to(squares, (slots, squares_ref.shape[1]))
    for piece in range(pieces):
        factor = jnp.concatenate(factors[piece], axis=0) if last else None
        for start in range(0, ff, tile):
            columns = slice(start, start + tile)
            pair = []
            for kind, ref in enumerate((gate_ref, up_ref)):
                value = jnp.dot(
                    normed[piece],
                    ref[piece, pl.ds(base, depth), columns],
                    preferred_element_type=F32,
                )
                if last:
                    pair.append((value + sums_ref[kind, piece, :, columns]) * factor)
                else:
                    sums_ref[kind, piece, :, columns] = value
            if last:
                gate = jnp.minimum(pair[0], CLAMP_LIMIT)
                up = jnp.clip(pair[1], -CLAMP_LIMIT, CLAMP_LIMIT)
                hidden_ref[piece, :, columns] = (
                    (up + 1.0) * gate * jax.nn.sigmoid(GLU_ALPHA * gate)
                ).astype(BF16)
    if last:
        down_kernel(
            spot_ref, hidden_ref, down_ref, sent_ref, kept_ref,
            groups=groups, capacity=capacity, width=width, first=span,
        )


def hidden_units(spot, tables, prior, gain, gate, up, groups, capacity, width, chunk):
    pieces, _, ff = gate.shape
    rows, depth = groups * capacity, CORES * tables[0].shape[1]
    last = prior is not None
    sums = [shape_of(2, pieces, rows, ff, dtype=F32), shape_of(pieces * rows, 128, dtype=F32)]
    outs = [shape_of(pieces, rows, ff)] + [shape_of(pieces * rows, depth // CORES)] * 2
    inputs = list(tables) + [gain[None, :], gate, up] + (list(prior) if last else [])
    return pl.pallas_call(
        functools.partial(
            hidden_kernel, groups=groups, capacity=capacity, width=width, chunk=chunk, last=last
        ),
        out_shape=outs if last else sums,
        in_specs=[scalars()] + [whole()] * len(inputs),
        out_specs=[whole()] * len(outs if last else sums),
        scratch_shapes=[pltpu.VMEM((pieces, rows, depth), BF16)],
        cost_estimate=cost(
            4 * pieces * rows * depth * ff, 4 * pieces * depth * (ff + rows), pieces * rows * ff
        ),
        compiler_params=grant(16),
    )(spot, *inputs)


def down_kernel(
    spot_ref, hidden_ref, down_ref, sent_ref, kept_ref, *, groups, capacity, width, first
):
    pieces = hidden_ref.shape[0]
    for side, ref in ((1, sent_ref), (0, kept_ref)):
        for piece in range(pieces):
            for inner in range(ref.shape[1] // width):
                start = block_start(spot_ref, first + inner, side, width)
                value = jnp.dot(
                    hidden_ref[piece],
                    down_ref[piece, :, pl.ds(pl.multiple_of(start, width), width)],
                    preferred_element_type=F32,
                ).astype(BF16)
                for group in range(groups):
                    row = (group * pieces + piece) * capacity
                    ref[row : row + capacity, inner * width : (inner + 1) * width] = value[
                        group * capacity : (group + 1) * capacity
                    ]


def down(spot, hidden, down_weight, groups, capacity, width, first, span):
    pieces, rows, ff = hidden.shape
    part = span * width
    return pl.pallas_call(
        functools.partial(down_kernel, groups=groups, capacity=capacity, width=width, first=first),
        out_shape=[shape_of(pieces * rows, part)] * 2,
        in_specs=[scalars(), whole(), whole()],
        out_specs=[whole()] * 2,
        cost_estimate=cost(
            2 * CORES * pieces * rows * ff * part, 2 * CORES * pieces * part * (ff + rows)
        ),
        compiler_params=grant(12),
        name="down",
    )(spot, hidden, down_weight)


def add_kernel(kept_ref, partner_ref, *out_refs):
    rows = out_refs[0].shape[0]
    for group, ref in enumerate(out_refs):
        place = slice(group * rows, (group + 1) * rows)
        ref[...] = (kept_ref[place].astype(F32) + partner_ref[place].astype(F32)).astype(BF16)


def add_cores(kept, partner, groups):
    rows, width = kept.shape
    return pl.pallas_call(
        add_kernel,
        out_shape=[shape_of(rows // groups, width)] * groups,
        in_specs=[whole()] * 2,
        out_specs=[whole()] * groups,
        cost_estimate=cost(2**21, 6 * rows * width),
        compiler_params=grant(6),
        name="add_cores",
    )(kept, partner)


def part_kernel(kept_ref, partner_ref, mine_ref, *out_refs):
    width = mine_ref.shape[1]
    for level, ref in enumerate((mine_ref,) + out_refs):
        place = slice(level * width, (level + 1) * width)
        total = kept_ref[:, place].astype(F32) + partner_ref[:, place].astype(F32)
        ref[...] = total.astype(ref.dtype)


def part_levels(kept, partner, levels):
    rows, width = kept.shape
    own = width // levels
    return pl.pallas_call(
        part_kernel,
        out_shape=[shape_of(rows, own, dtype=F32)] + [shape_of(rows, own)] * (levels - 1),
        in_specs=[whole()] * 2,
        out_specs=[whole()] * levels,
        cost_estimate=cost(2**21, 6 * rows * width),
        compiler_params=grant(6),
        name="part_levels",
    )(kept, partner)


def sum_kernel(*refs, groups):
    value_refs, out_refs = refs[:-groups], refs[-groups:]
    rows = out_refs[0].shape[0]
    for group, ref in enumerate(out_refs):
        place = slice(group * rows, (group + 1) * rows)
        total = value_refs[0][place]
        for value_ref in value_refs[1:]:
            total += value_ref[place].astype(F32)
        ref[...] = total.astype(BF16)


def sum_levels(values, groups):
    rows, width = values[0].shape
    return pl.pallas_call(
        functools.partial(sum_kernel, groups=groups),
        out_shape=[shape_of(rows // groups, width)] * groups,
        in_specs=[whole()] * len(values),
        out_specs=[whole()] * groups,
        cost_estimate=cost(2**21, 6 * rows * width),
        compiler_params=grant(6),
        name="sum_levels",
    )(*values)


def plan_kernel(
    place_ref, routes_ref, weights_ref, out_ref, scale_ref, *, capacity, pieces, experts
):
    picks, rows = routes_ref.shape
    slots = out_ref.shape[2]
    groups = out_ref.shape[0] // picks
    wide = max(experts, 128)
    first = lax.broadcasted_iota(jnp.int32, (rows, rows), 0)
    second = lax.broadcasted_iota(jnp.int32, (rows, rows), 1)

    def column(row):
        return jnp.sum(jnp.where(first == second, row, 0.0), axis=1, keepdims=True)

    expert = lax.broadcasted_iota(jnp.int32, (rows, wide), 1)
    named = jnp.zeros((rows, wide), jnp.bool_)
    scale = jnp.zeros((rows, scale_ref.shape[1]), F32)
    lane = lax.broadcasted_iota(jnp.int32, scale.shape, 1)
    routes = []
    for pick in range(picks):
        routes.append(column(routes_ref[pick : pick + 1, :].astype(F32)).astype(jnp.int32))
        named = named | (routes[pick] == expert)
        scale = jnp.where(lane == pick, column(weights_ref[pick : pick + 1, :]), scale)
    scale_ref[...] = scale
    rank = ranks(named, second < first, 0)
    slot = lax.broadcasted_iota(jnp.int32, (rows, slots), 1)
    for pick in range(picks):
        mine = jnp.sum(jnp.where(expert == routes[pick], rank, 0.0), axis=1, keepdims=True)
        target = routes[pick] * capacity + mine.astype(jnp.int32)
        for mask in range(groups):
            here = slot + jnp.bitwise_xor(place_ref[0], mask) * slots
            out_ref[pick * groups + mask] = (here == target).astype(F32).astype(BF16)


def plan(place, routes, route_weights, capacity, pieces, experts, groups):
    picks, rows = routes.shape
    slots = pieces * capacity
    return pl.pallas_call(
        functools.partial(plan_kernel, capacity=capacity, pieces=pieces, experts=experts),
        out_shape=[shape_of(picks * groups, rows, slots), shape_of(rows, 128, dtype=F32)],
        in_specs=[scalars(), whole(), whole()],
        out_specs=[whole()] * 2,
        cost_estimate=cost(2**25, 2 * picks * groups * rows * slots),
        compiler_params=grant(6, groups),
        name="plan",
    )(place, routes, route_weights)


def gather_rows(chosen_ref, scale_ref, table_refs):
    groups = len(table_refs)
    total = None
    for pick in range(chosen_ref.shape[0] // groups):
        picked = None
        for group in range(groups):
            part = jnp.dot(
                chosen_ref[pick * groups + group],
                table_refs[group][...],
                preferred_element_type=F32,
            )
            picked = part if picked is None else picked + part
        picked = picked * scale_ref[:, pick : pick + 1]
        total = picked if total is None else total + picked
    return total


def gather_kernel(chosen_ref, scale_ref, *refs, groups):
    total = gather_rows(chosen_ref, scale_ref, refs[:groups])
    out_refs = refs[groups:]
    width = out_refs[0].shape[1]
    for level, ref in enumerate(out_refs):
        ref[...] = total[:, level * width : (level + 1) * width].astype(BF16)


def gather(chosen, scale, tables, levels):
    groups = len(tables)
    rows, picks = scale.shape[0], chosen.shape[0] // groups
    slots, width = tables[0].shape
    return pl.pallas_call(
        functools.partial(gather_kernel, groups=groups),
        out_shape=[shape_of(rows, width // levels)] * levels,
        in_specs=[whole()] * (2 + groups),
        out_specs=[whole()] * levels,
        cost_estimate=cost(
            2 * picks * groups * slots * rows * width,
            2 * groups * slots * (width + picks * rows) + 2 * rows * width,
        ),
        compiler_params=grant(8),
        name="gather",
    )(chosen, scale, *tables)


def final_kernel(chosen_ref, scale_ref, *refs, groups):
    total = gather_rows(chosen_ref, scale_ref, refs[:groups])
    for ref in refs[groups:-1]:
        total += ref[...].astype(F32)
    refs[-1][...] = total.astype(BF16)


def final(chosen, scale, tables, parts):
    rows, width = parts[0].shape
    groups = len(tables)
    return pl.pallas_call(
        functools.partial(final_kernel, groups=groups),
        out_shape=shape_of(rows, width),
        in_specs=[whole()] * (2 + groups + len(parts)),
        out_specs=whole(),
        cost_estimate=cost(2**28, 2 * (groups + len(parts)) * rows * width),
        compiler_params=grant(8),
        name="final",
    )(chosen, scale, *tables, *parts)


def shards(
    queries, keys, values, mix_weight, sub_gain, tokens, routes, route_weights,
    expert_gain, gate_weight, up_weight, down_weight,
):
    rows2, width = tokens.shape
    picks = routes.shape[1]
    groups, levels = lax.axis_size("ep"), lax.axis_size("tp") // CORES
    pieces = gate_weight.shape[0]
    experts = groups * pieces
    capacity = 3 * rows2 * picks // (2 * experts)
    half = levels // 2
    tp_index = lax.axis_index("tp")
    spot = jnp.stack([lax.axis_index("ep"), tp_index // CORES, tp_index % CORES])
    place = spot = spot.astype(jnp.int32)

    by_level = [tokens]
    for mask in range(1, levels):
        by_level.append(levels_flip(tokens, mask))
    (gate_near,) = fetch(gate_weight, mebibytes=GATE_GRANT)
    by_level[0], picked, picked_weights = fetch(tokens, routes.T, route_weights.T, mebibytes=2)
    chosen, scale = plan(
        place, picked, picked_weights, capacity, pieces, experts, groups
    )
    queries, keys, values, scale = lax.optimization_barrier((queries, keys, values, scale))
    bundles = pack(place, queries, keys, values, groups)
    own, other = [], []
    for chunk in range(2):
        some = by_level[chunk * half : (chunk + 1) * half]
        tables = dispatch(place, picked, some, capacity, pieces, experts, groups)
        own.append(exchange(tables))
    bundles = exchange(bundles)
    for chunk in range(2):
        swapped = []
        for table in own[chunk]:
            swapped.append(cores_flip(table))
        other.append(swapped)
    (up_near,) = fetch(up_weight, mebibytes=UP_GRANT)
    hidden = None
    for chunk in range(2):
        if chunk == 1:
            hidden = list(hidden) + [down_weight]
        hidden = hidden_units(
            spot, own[chunk] + other[chunk], hidden, expert_gain, gate_near, up_near,
            groups, capacity, width, chunk,
        )
    hidden, sent, kept = hidden
    halves = [(kept, cores_flip(sent))]
    sent, kept = down(spot, hidden, down_weight, groups, capacity, width, 0, half)
    halves.insert(0, (kept, cores_flip(sent)))
    values = list(part_levels(*halves[0], half))
    for level in range(1, half):
        values[level] = levels_flip(values[level], level)
    tables = add_cores(*halves[1], groups)
    tables = exchange(tables)
    combined = gather(chosen, scale, tables, half)
    results = []
    for inner, value in enumerate(combined):
        results.append(levels_flip(value, half + inner))
    tables = sum_levels(values, groups)
    tables = exchange(tables)
    attended = attention(place, bundles, mix_weight, sub_gain, queries.shape[0])
    attended = exchange(attended)
    moe_out = final(chosen, scale, tables, results)
    attn_out = unpack(place, attended, queries.shape[1])
    return (attn_out, moe_out)


def solution(mesh):
    return jax.shard_map(
        shards,
        mesh=mesh,
        in_specs=(
            P("ep", "tp", None),
            P("ep", "tp", None),
            P("ep", "tp", None),
            P("tp"),
            P(),
            P("ep", "tp"),
            P("ep", None),
            P("ep", None),
            P(),
            P("ep", None, "tp"),
            P("ep", None, "tp"),
            P("ep", "tp", None),
        ),
        out_specs=(P("ep", "tp", None), P("ep", "tp")),
        check_vma=False,
    )
```
